256 devices in a mesh: fs: 32 (over z, x), tp: 8 (over y, core).
Axes of the slice: x: 4, y: 4, z: 8, core: 2. Of those that a mesh axis runs over, the one named last changes fastest.
Arguments:
- tokens: bfloat16 [16384, 2048], P('fs', 'tp'), may hold values from -16 to 16
- pre_mix_gain: bfloat16 [2048], P('tp'), may hold values from 0.099609375 to 1.8984375
- w_gate_in: bfloat16 [2048, 2048], P('fs', 'tp'), may hold values from -0.125 to 0.125
- w_input: bfloat16 [2048, 2048], P('fs', 'tp'), may hold values from -0.125 to 0.125
- mix_kernel: bfloat16 [4, 2048], P(None, 'tp'), may hold values from -3 to 3
- w_recur: bfloat16 [8, 256, 256], P('tp'), may hold values from -0.375 to 0.375
- w_inject: bfloat16 [8, 256, 256], P('tp'), may hold values from -0.375 to 0.375
- decay_param: float32 [2048], P('tp'), may hold values from 3 to 13
- w_mix_out: bfloat16 [2048, 2048], P('tp', 'fs'), may hold values from -0.125 to 0.125
- post_mix_gain: bfloat16 [2048], P('tp'), may hold values from 0.099609375 to 1.8984375
- pre_ffn_gain: bfloat16 [2048], P('tp'), may hold values from 0.099609375 to 1.8984375
- w_up_gate: bfloat16 [2048, 5632], P('fs', 'tp'), may hold values from -0.125 to 0.125
- w_up_value: bfloat16 [2048, 5632], P('fs', 'tp'), may hold values from -0.125 to 0.125
- gate_kernel: bfloat16 [3, 5632], P(None, 'tp'), may hold values from -3 to 3
- value_kernel: bfloat16 [3, 5632], P(None, 'tp'), may hold values from -3 to 3
- w_down: bfloat16 [5632, 2048], P('tp', 'fs'), may hold values from -0.078125 to 0.078125
- post_ffn_gain: bfloat16 [2048], P('tp'), may hold values from 0.099609375 to 1.8984375
Outputs:
- layer_out: bfloat16 [16384, 2048], P('fs', 'tp')
The draws below stay inside these ranges and needn't reach their ends.
All inputs are finite; a program needn't handle non-finite values.
Results may differ from the reference program's by a relative error of at most 0.015.
Values may be sent and summed in bfloat16 or wider, within the bound.
No kernel may reach another device: no remote copies, remote signals or barrier semaphores. Data moves between devices by JAX's collectives and lax.ppermute only.
A program may use at most 64 MiB of HBM per device.

```python
import math
import jax
import jax.numpy as jnp
from jax import lax

D = 2048
HEADS = 8
HEAD_SIZE = 256
W = 2048
FF = 5632
MIX_TAPS = 4
FFN_TAPS = 3
LEN = 512
TOKENS = 16384
N_FS = 32
N_TP = 8


gate_power = 8.0


def draw_tokens(key, part):
    keys = jax.random.split(key, 6)
    levels = 0.5 * 4.0 ** (jnp.arange(8, dtype=jnp.float32) / 7.0)
    order = jax.random.permutation(keys[0], 8)
    channel_scale = levels[order][jnp.arange(D) // (D // 8)]
    noise = jax.random.normal(keys[1], (TOKENS, D), jnp.float32)
    direction = jax.random.normal(keys[2], (D,), jnp.float32)
    shift = jax.random.normal(keys[3], (TOKENS // 16, 1), jnp.float32) * 1.5
    shift = jnp.repeat(shift, 16, axis=0)
    values = noise * channel_scale[None, :] + shift * direction[None, :]
    return jnp.clip(values, -16.0, 16.0).astype(jnp.bfloat16)


def draw_decay_param(key, part):
    keys = jax.random.split(key, 3)
    slow = jnp.exp(jax.random.uniform(keys[0], (W,), jnp.float32, math.log(0.1), math.log(2.0))) / (gate_power * LEN)
    fast = jnp.exp(jax.random.uniform(keys[1], (W,), jnp.float32, math.log(0.01), math.log(0.04)))
    picks = jax.random.randint(keys[2], (W,), 0, 2) == 1
    rate = jnp.where(picks, fast, slow)
    return (-jnp.log(jnp.expm1(rate))).astype(jnp.float32)


def steps_of(stream_key, shape, cuts, low, largest):
    loudness, own = 1.0, jax.random.fold_in(stream_key, 6)
    for axis_at, parts in cuts:
        draws = jnp.exp(jax.random.uniform(jax.random.fold_in(own, axis_at), (parts,), jnp.float32, low / len(cuts), largest / len(cuts)))
        loudness = loudness * jnp.repeat(draws, shape[axis_at] // parts).reshape([-1 if axis == axis_at else 1 for axis in range(len(shape))])
    return loudness


def centred(rng, dims, spread, reach, cuts=(), held_as=jnp.bfloat16):
    values = jax.random.normal(rng, dims, jnp.float32) * spread
    if len(cuts) > 0:
        values = steps_of(rng, dims, cuts, -0.22, 0.18) * values
    return jnp.clip(values, min=-reach, max=reach).astype(held_as)


def setup_inputs(seed: int = 0) -> dict:
    arg_keys = jax.random.split(jax.random.key(seed), 18)
    return {
        "tokens": draw_tokens(jax.random.fold_in(arg_keys[17], 71), 0),
        "pre_mix_gain": jnp.clip(1.0 + 0.18 * jax.random.normal(arg_keys[1], (D,), jnp.float32), 0.099609375, 1.8984375).astype(jnp.bfloat16),
        "w_gate_in": centred(arg_keys[2], (D, W), D ** -0.5, 0.125, ((0, 32), (1, 8))),
        "w_input": centred(arg_keys[3], (D, W), D ** -0.5, 0.125, ((0, 32), (1, 8))),
        "mix_kernel": centred(arg_keys[4], (MIX_TAPS, W), 0.5, 3.0, ((1, 8),)),
        "w_recur": centred(arg_keys[5], (HEADS, HEAD_SIZE, HEAD_SIZE), HEAD_SIZE ** -0.5, 0.375, ((0, 8),)),
        "w_inject": centred(arg_keys[6], (HEADS, HEAD_SIZE, HEAD_SIZE), HEAD_SIZE ** -0.5, 0.375, ((0, 8),)),
        "decay_param": draw_decay_param(jax.random.fold_in(arg_keys[17], 71), 0),
        "w_mix_out": centred(arg_keys[8], (W, D), W ** -0.5, 0.125, ((0, 8), (1, 32))),
        "post_mix_gain": jnp.clip(1.0 + 0.18 * jax.random.normal(arg_keys[9], (D,), jnp.float32), 0.099609375, 1.8984375).astype(jnp.bfloat16),
        "pre_ffn_gain": jnp.clip(1.0 + 0.18 * jax.random.normal(arg_keys[10], (D,), jnp.float32), 0.099609375, 1.8984375).astype(jnp.bfloat16),
        "w_up_gate": centred(arg_keys[11], (D, FF), D ** -0.5, 0.125, ((0, 32), (1, 8))),
        "w_up_value": centred(arg_keys[12], (D, FF), D ** -0.5, 0.125, ((0, 32), (1, 8))),
        "gate_kernel": centred(arg_keys[13], (FFN_TAPS, FF), 0.577, 3.0, ((1, 8),)),
        "value_kernel": centred(arg_keys[14], (FFN_TAPS, FF), 0.577, 3.0, ((1, 8),)),
        "w_down": centred(arg_keys[15], (FF, D), FF ** -0.5, 0.078125, ((0, 8), (1, 32))),
        "post_ffn_gain": jnp.clip(1.0 + 0.18 * jax.random.normal(arg_keys[16], (D,), jnp.float32), 0.099609375, 1.8984375).astype(jnp.bfloat16),
    }


norm_eps = 1e-06
gate_power = 8.0

def row_normed(values, row_gain):
    widened = values.astype(jnp.float32)
    squares = lax.optimization_barrier(jnp.sum(widened * widened, axis=1))
    factor = lax.rsqrt(squares / D + norm_eps)
    return widened * factor[:, None] * row_gain.astype(jnp.float32)[None, :]

def causal_conv(values, kernel):
    length = values.shape[0]
    widths = kernel.shape[0]
    padded = jnp.pad(values.astype(jnp.float32), ((widths - 1, 0), (0, 0)))
    weights = kernel.astype(jnp.float32)
    result = padded[0:length] * weights[0]
    for offset in range(1, widths):
        result = result + padded[offset:offset + length] * weights[offset]
    return result

def linear_combine(earlier, latter):
    return (earlier[0] * latter[0], latter[0] * earlier[1] + latter[1])

def split_sum(activ, weight):
    length = activ.shape[0]
    blocks = activ.reshape(length, N_TP, -1).transpose(1, 0, 2).astype(jnp.float32)
    wblocks = weight.reshape(N_TP, -1, weight.shape[1]).astype(jnp.float32)
    partial_value = jnp.einsum('ktw,kwd->ktd', blocks, wblocks)
    partial_value = partial_value.astype(jnp.bfloat16).astype(jnp.float32)
    return lax.optimization_barrier(jnp.sum(partial_value, axis=0))

def reference(tokens, pre_mix_gain, w_gate_in, w_input, mix_kernel, w_recur, w_inject, decay_param, w_mix_out, post_mix_gain, pre_ffn_gain, w_up_gate, w_up_value, gate_kernel, value_kernel, w_down, post_ffn_gain):
    sequences = tokens.reshape(N_FS, LEN, D)

    def one_sequence(rows):
        normed_in = row_normed(rows, pre_mix_gain).astype(jnp.bfloat16)
        gate_rows = jnp.dot(normed_in, w_gate_in, preferred_element_type=jnp.float32).astype(jnp.bfloat16)
        input_rows = jnp.dot(normed_in, w_input, preferred_element_type=jnp.float32).astype(jnp.bfloat16)
        smoothed = causal_conv(input_rows, mix_kernel).astype(jnp.bfloat16)
        by_head = smoothed.reshape(LEN, HEADS, HEAD_SIZE).astype(jnp.float32)
        recur_gate = jax.nn.sigmoid(jnp.einsum('thi,hij->thj', by_head, w_recur.astype(jnp.float32))).reshape(LEN, W)
        inject_gate = jax.nn.sigmoid(jnp.einsum('thi,hij->thj', by_head, w_inject.astype(jnp.float32))).reshape(LEN, W)
        log_retain = -gate_power * recur_gate * jax.nn.softplus(-decay_param.astype(jnp.float32))[None, :]
        retain = jnp.exp(log_retain)
        driven = jnp.sqrt(-jnp.expm1(2.0 * log_retain)) * inject_gate * smoothed.astype(jnp.float32)
        _, states = lax.associative_scan(linear_combine, (retain, driven), axis=0)
        hidden = (jax.nn.gelu(gate_rows.astype(jnp.float32), approximate=True) * states).astype(jnp.bfloat16)
        mixer_sum = split_sum(hidden, w_mix_out)
        middle = (rows.astype(jnp.float32) + row_normed(mixer_sum, post_mix_gain)).astype(jnp.bfloat16)
        normed_mid = row_normed(middle, pre_ffn_gain).astype(jnp.bfloat16)
        up_gate = jnp.dot(normed_mid, w_up_gate, preferred_element_type=jnp.float32).astype(jnp.bfloat16)
        up_value = jnp.dot(normed_mid, w_up_value, preferred_element_type=jnp.float32).astype(jnp.bfloat16)
        conv_g = causal_conv(up_gate, gate_kernel)
        conv_v = causal_conv(up_value, value_kernel)
        activated = (jax.nn.gelu(conv_g, approximate=True) * conv_v).astype(jnp.bfloat16)
        ffn_sum = split_sum(activated, w_down)
        return (middle.astype(jnp.float32) + row_normed(ffn_sum, post_ffn_gain)).astype(jnp.bfloat16)
    return lax.map(one_sequence, sequences).reshape(N_FS * LEN, D)
```

```python
import functools
import jax
import jax.numpy as jnp
from jax import lax
from jax.experimental import pallas as pl
from jax.experimental.pallas import tpu as pltpu
from jax.sharding import Mesh
from jax.sharding import PartitionSpec as P

D = 2048
FS = ("z", "x")
TP = ("y", "c")
NZ, NX, NTP = 8, 4, 8
ROWS = 512
OWN = ROWS // NTP
PIECE = D // NTP
norm_eps = 1e-06
gate_power = 8.0
bf16, f32 = jnp.bfloat16, jnp.float32


def sent_to_all(shard, axis, devices):
    return lax.all_to_all(
        jnp.broadcast_to(shard[None], (devices, *shard.shape)), axis, 0, 0, tiled=True
    )


def row_normed(values, row_gain):
    widened = values.astype(f32)
    factor = lax.rsqrt(jnp.sum(widened * widened, axis=1, keepdims=True) / D + norm_eps)
    return widened * factor * row_gain.astype(f32)


def gelu(v):
    return 0.5 * v * (1.0 + jnp.tanh(0.7978845608028654 * (v + 0.044715 * v * v * v)))


def one_less_exp(u):
    s = 1.0 + u * (1.0 / 8.0)
    for k in range(7, 1, -1):
        s = 1.0 + u * (1.0 / k) * s
    return jnp.where(u > -0.5, -u * s, 1.0 - jnp.exp(u))


def shifted_down(values, by, rows):
    return jnp.where(rows >= by, pltpu.roll(values, by, 0), 0.0)


def mixer_kernel(
    x_ref, w_ref, taps_ref, recur_ref, inject_ref, slope_ref, o_ref,
    win_ref, wout_ref, keep_ref, drive_ref,
):
    for z in range(NZ):
        for x in range(NX):
            at = (z * NX + x) * 64
            win_ref[at : at + 64, :] = w_ref[x, z, :, 0:512]
            wout_ref[at : at + 64, :] = w_ref[x, z, :, 512:768]
    squares = jnp.zeros((ROWS, 1), f32)
    for k in range(NTP):
        v = x_ref[k, 0:ROWS, :].astype(f32)
        squares = squares + jnp.sum(v * v, axis=1, keepdims=True)
    factor = lax.rsqrt(squares / D + norm_eps)
    both = jnp.zeros((ROWS, 2 * PIECE), f32)
    for k in range(NTP):
        gain = x_ref[k, ROWS : ROWS + 1, :].astype(f32)
        v = (x_ref[k, 0:ROWS, :].astype(f32) * factor * gain).astype(bf16)
        both = both + jnp.dot(
            v, win_ref[k * PIECE : (k + 1) * PIECE, :], preferred_element_type=f32
        )
    gate_rows = both[:, 0:PIECE].astype(bf16)
    input_rows = both[:, PIECE:].astype(bf16).astype(f32)
    rows = lax.broadcasted_iota(jnp.int32, (ROWS, PIECE), 0)
    taps = taps_ref[...].astype(f32)
    smoothed = input_rows * taps[3:4, :]
    for back in (1, 2, 3):
        smoothed = smoothed + shifted_down(input_rows, back, rows) * taps[3 - back : 4 - back, :]
    smoothed = smoothed.astype(bf16)
    recur = jax.nn.sigmoid(jnp.dot(smoothed, recur_ref[...], preferred_element_type=f32))
    inject = jax.nn.sigmoid(jnp.dot(smoothed, inject_ref[...], preferred_element_type=f32))
    log_retain = -gate_power * recur * slope_ref[...]
    keep = jnp.exp(log_retain)
    drive = jnp.sqrt(one_less_exp(2.0 * log_retain)) * inject * smoothed.astype(f32)
    within = rows % 8
    for by in (1, 2, 4):
        ok = within >= by
        drive = jnp.where(ok, keep * pltpu.roll(drive, by, 0), 0.0) + drive
        keep = jnp.where(ok, pltpu.roll(keep, by, 0), 1.0) * keep
    keep_ref[...] = keep
    drive_ref[...] = drive

    def tile(i, carry):
        at = pl.ds(pl.multiple_of(i * 8, 8), 8)
        state = keep_ref[at, :] * carry + drive_ref[at, :]
        drive_ref[at, :] = state
        return state[7:8, :]

    lax.fori_loop(0, ROWS // 8, tile, jnp.zeros((1, PIECE), f32), unroll=8)
    hidden = (gelu(gate_rows.astype(f32)) * drive_ref[...]).astype(bf16)
    for k in range(NTP):
        o_ref[:, k * PIECE : (k + 1) * PIECE] = lax.dot_general(
            hidden, wout_ref[k * PIECE : (k + 1) * PIECE, :], (((1,), (1,)), ((), ())),
            preferred_element_type=f32,
        ).astype(bf16)


def mixer(x_all, w_all, taps, w_recur, w_inject, slope):
    vmem = pl.BlockSpec(memory_space=pltpu.VMEM)
    return pl.pallas_call(
        mixer_kernel,
        out_shape=jax.ShapeDtypeStruct((ROWS, D), bf16),
        in_specs=[vmem] * 6,
        out_specs=vmem,
        scratch_shapes=[
            pltpu.VMEM((D, 512), bf16),
            pltpu.VMEM((D, PIECE), bf16),
            pltpu.VMEM((ROWS, PIECE), f32),
            pltpu.VMEM((ROWS, PIECE), f32),
        ],
        compiler_params=pltpu.CompilerParams(vmem_limit_bytes=40 * 1024 * 1024),
        cost_estimate=pl.CostEstimate(
            flops=2 * ROWS * D * 768 + 4 * ROWS * PIECE * PIECE,
            bytes_accessed=8 * 1024 * 1024, transcendentals=ROWS * PIECE * 6,
        ),
        name="mixer",
    )(x_all, w_all, taps, w_recur, w_inject, slope)


def causal_conv(values, kernel):
    length = values.shape[0]
    widths = kernel.shape[0]
    padded = jnp.pad(values.astype(f32), ((widths - 1, 0), (0, 0)))
    weights = kernel.astype(f32)
    result = padded[0:length] * weights[0]
    for offset in range(1, widths):
        result = result + padded[offset : offset + length] * weights[offset]
    return result


def summed(pieces):
    return jnp.sum(pieces.astype(f32), axis=0)


def shards(
    tokens, pre_mix_gain, w_gate_in, w_input, mix_kernel, w_recur, w_inject, decay_param,
    w_mix_out, post_mix_gain, pre_ffn_gain, w_up_gate, w_up_value, gate_kernel, value_kernel,
    w_down, post_ffn_gain,
):
    ffn_own = jnp.concatenate([w_up_gate, w_up_value, w_down.T], axis=1)
    ffn_all = lax.all_gather(ffn_own, FS, axis=0, tiled=True)
    up_gate_all, up_value_all, down_all = jnp.split(ffn_all, [704, 1408], axis=1)

    gains = jnp.stack([pre_mix_gain, post_mix_gain, pre_ffn_gain, post_ffn_gain])
    packed = jnp.concatenate([tokens, jnp.pad(gains, ((0, 12), (0, 0)))], axis=0)
    mix_own = jnp.concatenate([w_gate_in, w_input, w_mix_out.T], axis=1)
    mix_z = sent_to_all(mix_own, "z", NZ)
    x_all = sent_to_all(packed, TP, NTP)
    mix_all = sent_to_all(mix_z.reshape(NZ, 64, 768), "x", NX).reshape(NX, NZ, 64, 768)
    x_all = x_all.reshape(NTP, ROWS + 16, PIECE)
    slope = jax.nn.softplus(-decay_param)[None, :]
    partial_mix = mixer(x_all, mix_all, mix_kernel, w_recur[0], w_inject[0], slope)

    me = lax.axis_index("y") * 2 + lax.axis_index("c")
    own_rows = lax.dynamic_slice(x_all, (0, me * OWN, 0), (NTP, OWN, PIECE))
    own_rows = own_rows.transpose(1, 0, 2).reshape(OWN, D)
    full_gains = x_all[:, ROWS : ROWS + 4, :].transpose(1, 0, 2).reshape(4, D)

    mixer_sum = summed(lax.all_to_all(partial_mix.reshape(NTP, OWN, D), TP, 0, 0, tiled=True))
    middle = (own_rows.astype(f32) + row_normed(mixer_sum, full_gains[1:2])).astype(bf16)
    normed_own = row_normed(middle, full_gains[2:3]).astype(bf16)
    normed_mid = sent_to_all(normed_own, TP, NTP).reshape(ROWS, D)

    up_gate = jnp.dot(normed_mid, up_gate_all, preferred_element_type=f32).astype(bf16)
    up_value = jnp.dot(normed_mid, up_value_all, preferred_element_type=f32).astype(bf16)
    conv_g = causal_conv(up_gate, gate_kernel)
    conv_v = causal_conv(up_value, value_kernel)
    activated = (jax.nn.gelu(conv_g, approximate=True) * conv_v).astype(bf16)
    partial_ffn = lax.dot_general(
        activated, down_all, (((1,), (1,)), ((), ())), preferred_element_type=f32
    ).astype(bf16)
    ffn_sum = summed(lax.all_to_all(partial_ffn.reshape(NTP, OWN, D), TP, 0, 0, tiled=True))
    out_rows = (middle.astype(f32) + row_normed(ffn_sum, full_gains[3:4])).astype(bf16)
    to_columns = out_rows.reshape(OWN, NTP, PIECE).transpose(1, 0, 2)
    return lax.all_to_all(to_columns, TP, 0, 0, tiled=True).reshape(ROWS, PIECE)


def solution(mesh):
    finer = Mesh(mesh.devices.reshape(NZ, NX, 4, 2), ("z", "x", "y", "c"))
    return jax.shard_map(
        shards,
        mesh=finer,
        in_specs=(
            P(FS, TP), P(TP), P(FS, TP), P(FS, TP), P(None, TP), P(TP, None, None),
            P(TP, None, None), P(TP), P(TP, FS), P(TP), P(TP), P(FS, TP), P(FS, TP),
            P(None, TP), P(None, TP), P(TP, FS), P(TP),
        ),
        out_specs=P(FS, TP),
        check_vma=False,
    )
```

```python
import jax
import jax.numpy as jnp
from jax import lax
from jax.experimental import pallas as pl
from jax.experimental.pallas import tpu as pltpu
from jax.sharding import Mesh
from jax.sharding import PartitionSpec as P

D = 2048
FS = ("z", "x")
TP = ("y", "c")
NZ, NX, NY, NC = 8, 4, 4, 2
NTP = NY * NC
ROWS = 512
OWN = ROWS // NTP
PIECE = D // NTP
EXTRA = 16
UNITS = 704
norm_eps = 1e-06
gate_power = 8.0
bf16, f32 = jnp.bfloat16, jnp.float32


def moved(value, axis, n, by):
    return lax.ppermute(value, axis, [(i, (i + by) % n) for i in range(n)])


def ring_gathered(block, axis, n):
    got = [block] + [None] * (n - 1)
    ahead = back = block
    for s in range(1, n // 2):
        ahead = moved(ahead, axis, n, 1)
        back = moved(back, axis, n, -1)
        got[s], got[n - s] = ahead, back
    half = block.shape[0] // 2
    first = moved(ahead[:half], axis, n, 1)
    second = moved(back[half:], axis, n, -1)
    got[n // 2] = jnp.concatenate([first, second], axis=0)
    return got


def swapped(value):
    return lax.ppermute(value, "c", [(0, 1), (1, 0)])


def tp_gathered(block):
    near = ring_gathered(block, "y", NY)
    return [v for b in near for v in (b, swapped(b))]


def summed_rows(mine, theirs):
    half = OWN // 2
    far = mine[2].astype(f32) + swapped(theirs[2]).astype(f32)
    far = far.astype(bf16)
    first = moved(far[:half], "y", NY, 1)
    second = moved(far[half:], "y", NY, -1)
    one = mine[1].astype(f32) + swapped(theirs[1]).astype(f32)
    back = mine[3].astype(f32) + swapped(theirs[3]).astype(f32)
    own = mine[0].astype(f32) + swapped(theirs[0]).astype(f32)
    one = jnp.concatenate([one[:half] + first.astype(f32), one[half:]], axis=0).astype(bf16)
    back = jnp.concatenate([back[:half], back[half:] + second.astype(f32)], axis=0).astype(bf16)
    return own + moved(one, "y", NY, 1).astype(f32) + moved(back, "y", NY, -1).astype(f32)


def row_normed(values, row_gain):
    widened = values.astype(f32)
    factor = lax.rsqrt(jnp.sum(widened * widened, axis=1, keepdims=True) / D + norm_eps)
    return widened * factor * row_gain.astype(f32)


def gelu(v):
    return 0.5 * v * (1.0 + jnp.tanh(0.7978845608028654 * (v + 0.044715 * v * v * v)))


def one_less_exp(u):
    s = 1.0 + u * (1.0 / 8.0)
    for k in range(7, 1, -1):
        s = 1.0 + u * (1.0 / k) * s
    return jnp.where(u > -0.5, -u * s, 1.0 - jnp.exp(u))


def shifted_down(values, by, rows):
    return jnp.where(rows >= by, pltpu.roll(values, by, 0), 0.0)


def stretch(index, size):
    return pl.ds(pl.multiple_of(index * size, size), size)


def behind(me, by, n):
    return lax.rem(me + (n - by), n)


def dot_nt(a, b):
    return lax.dot_general(a, b, (((1,), (1,)), ((), ())), preferred_element_type=f32)


def mixer_kernel(*refs):
    x_refs, gate_refs, in_refs, out_refs = refs[0:8], refs[8:16], refs[16:20], refs[20:24]
    taps_ref, recur_ref, inject_ref, slope_ref = refs[24:28]
    mine_ref, theirs_ref, own_ref, gain_ref = refs[28:32]
    win_ref, wout_ref, keep_ref, drive_ref, hid_ref = refs[32:]
    mz, mx = lax.axis_index("z"), lax.axis_index("x")
    my, mc = lax.axis_index("y"), lax.axis_index("c")
    for dz in range(NZ):
        for dx in range(NX):
            at = stretch(behind(mz, dz, NZ) * NX + behind(mx, dx, NX), 64)
            win_ref[at, 0:PIECE] = gate_refs[dz][dx]
            win_ref[at, PIECE:] = in_refs[dx][dz]
            wout_ref[at, :] = out_refs[dx][dz]
    tp = [behind(my, d // 2, NY) * NC + (mc if d % 2 == 0 else 1 - mc) for d in range(NTP)]
    first_own = pl.multiple_of(mc * 256 + my * OWN, OWN)
    squares = jnp.zeros((ROWS, 1), f32)
    for k in range(NTP):
        v = x_refs[k][0:ROWS, :].astype(f32)
        squares = squares + jnp.sum(v * v, axis=1, keepdims=True)
        own_ref[:, stretch(tp[k], PIECE)] = x_refs[k][pl.ds(first_own, OWN), :]
        gain_ref[:, stretch(tp[k], PIECE)] = x_refs[k][ROWS : ROWS + 8, :]
    factor = lax.rsqrt(squares / D + norm_eps)
    both = jnp.zeros((ROWS, 2 * PIECE), f32)
    for k in range(NTP):
        gain = x_refs[k][ROWS : ROWS + 1, :].astype(f32)
        v = (x_refs[k][0:ROWS, :].astype(f32) * factor * gain).astype(bf16)
        both = both + jnp.dot(v, win_ref[stretch(tp[k], PIECE), :], preferred_element_type=f32)
    gate_rows = both[:, 0:PIECE].astype(bf16)
    input_rows = both[:, PIECE:].astype(bf16).astype(f32)
    rows = lax.broadcasted_iota(jnp.int32, (ROWS, PIECE), 0)
    taps = taps_ref[...].astype(f32)
    smoothed = input_rows * taps[3:4, :]
    for back in (1, 2, 3):
        smoothed = smoothed + shifted_down(input_rows, back, rows) * taps[3 - back : 4 - back, :]
    smoothed = smoothed.astype(bf16)
    recur = jax.nn.sigmoid(jnp.dot(smoothed, recur_ref[...], preferred_element_type=f32))
    inject = jax.nn.sigmoid(jnp.dot(smoothed, inject_ref[...], preferred_element_type=f32))
    log_retain = -gate_power * recur * slope_ref[...]
    keep = jnp.exp(log_retain)
    drive = jnp.sqrt(one_less_exp(2.0 * log_retain)) * inject * smoothed.astype(f32)
    within = rows % 8
    for by in (1, 2, 4):
        ok = within >= by
        drive = jnp.where(ok, keep * pltpu.roll(drive, by, 0), 0.0) + drive
        keep = jnp.where(ok, pltpu.roll(keep, by, 0), 1.0) * keep
    keep_ref[...] = keep
    drive_ref[...] = drive

    def tile(i, carry):
        at = pl.ds(pl.multiple_of(i * 8, 8), 8)
        state = keep_ref[at, :] * carry + drive_ref[at, :]
        drive_ref[at, :] = state
        return state[7:8, :]

    lax.fori_loop(0, ROWS // 8, tile, jnp.zeros((1, PIECE), f32), unroll=8)
    hid_ref[...] = (gelu(gate_rows.astype(f32)) * drive_ref[...]).astype(bf16)
    projected(hid_ref, wout_ref, mine_ref, theirs_ref, my, mc)


def projected(hid_ref, wout_ref, mine_ref, theirs_ref, my, mc):
    for ref, half in ((theirs_ref, 1 - mc), (mine_ref, mc)):
        hidden = hid_ref[stretch(half, 256), :]
        for k in range(NTP):
            columns = slice(k * PIECE, (k + 1) * PIECE)
            part = dot_nt(hidden, wout_ref[columns, :]).astype(bf16)
            for y in range(NY):
                ref[lax.rem(y + NY - my, NY), :, columns] = part[y * OWN : (y + 1) * OWN, :]


VMEM = pl.BlockSpec(memory_space=pltpu.VMEM)
BY_ROWS = jax.ShapeDtypeStruct((NY, OWN, D), bf16)


def mixer(operands):
    return pl.pallas_call(
        mixer_kernel,
        out_shape=(
            BY_ROWS, BY_ROWS,
            jax.ShapeDtypeStruct((OWN, D), bf16), jax.ShapeDtypeStruct((8, D), bf16),
        ),
        in_specs=[VMEM] * len(operands),
        out_specs=(VMEM,) * 4,
        scratch_shapes=[
            pltpu.VMEM((D, 512), bf16),
            pltpu.VMEM((D, PIECE), bf16),
            pltpu.VMEM((ROWS, PIECE), f32),
            pltpu.VMEM((ROWS, PIECE), f32),
            pltpu.VMEM((ROWS, PIECE), bf16),
        ],
        compiler_params=pltpu.CompilerParams(vmem_limit_bytes=40 * 1024 * 1024),
        cost_estimate=pl.CostEstimate(
            flops=2 * ROWS * D * 768 + 4 * ROWS * PIECE * PIECE,
            bytes_accessed=8 * 1024 * 1024, transcendentals=ROWS * PIECE * 6,
        ),
        name="mixer",
    )(*operands)


UP_CUTS = [(0, 256), (256, 256), (512, 256), (768, 256), (1024, 256), (1280, 128)]


def ffn_kernel(*refs):
    n_refs = refs[0:8]
    w_ref, gtaps_ref, mine_ref, theirs_ref = refs[8:12]
    n_all, up_w, down_w, up_ref, act_ref, sems = refs[12:]
    my, mc = lax.axis_index("y"), lax.axis_index("c")
    copies = [
        pltpu.make_async_copy(
            w_ref.at[:, pl.ds(at, size)], up_w.at[:, pl.ds(at, size)], sems.at[i]
        )
        for i, (at, size) in enumerate(UP_CUTS)
    ]
    copies.append(
        pltpu.make_async_copy(w_ref.at[:, pl.ds(2 * UNITS, UNITS)], down_w, sems.at[len(UP_CUTS)])
    )
    for copy in copies:
        copy.start()
    for k in range(NTP):
        half = mc if k % 2 == 0 else 1 - mc
        n_all[stretch(half * NY + behind(my, k // 2, NY), OWN), :] = n_refs[k][...]
    for i, (at, size) in enumerate(UP_CUTS):
        copies[i].wait()
        up_ref[:, at : at + size] = jnp.dot(
            n_all[...], up_w[:, at : at + size], preferred_element_type=f32
        ).astype(bf16)
    taps = gtaps_ref[...].astype(f32)
    for at in range(0, ROWS, 128):
        if at == 0:
            v = up_ref[0:128, :].astype(f32)
            rows = lax.broadcasted_iota(jnp.int32, v.shape, 0)
            conv = v * taps[2:3, :]
            for back in (1, 2):
                conv = conv + shifted_down(v, back, rows) * taps[2 - back : 3 - back, :]
        else:
            v = up_ref[at - 16 : at + 128, :].astype(f32)
            conv = v[16:] * taps[2:3, :]
            for back in (1, 2):
                conv = conv + pltpu.roll(v, back, 0)[16:] * taps[2 - back : 3 - back, :]
        act_ref[at : at + 128, :] = (gelu(conv[:, 0:UNITS]) * conv[:, UNITS:]).astype(bf16)
    copies[-1].wait()
    projected(act_ref, down_w, mine_ref, theirs_ref, my, mc)


def ffn(blocks, w_all, taps):
    return pl.pallas_call(
        ffn_kernel,
        out_shape=(BY_ROWS, BY_ROWS),
        in_specs=[VMEM] * 8 + [pl.BlockSpec(memory_space=pl.ANY), VMEM],
        out_specs=(VMEM, VMEM),
        scratch_shapes=[
            pltpu.VMEM((ROWS, D), bf16),
            pltpu.VMEM((D, 2 * UNITS), bf16),
            pltpu.VMEM((D, UNITS), bf16),
            pltpu.VMEM((ROWS, 2 * UNITS), bf16),
            pltpu.VMEM((ROWS, UNITS), bf16),
            pltpu.SemaphoreType.DMA((len(UP_CUTS) + 1,)),
        ],
        compiler_params=pltpu.CompilerParams(vmem_limit_bytes=44 * 1024 * 1024),
        cost_estimate=pl.CostEstimate(
            flops=2 * ROWS * D * 3 * UNITS, bytes_accessed=13 * 1024 * 1024,
            transcendentals=ROWS * UNITS,
        ),
        name="ffn",
    )(*blocks, w_all, taps)


def shards(
    tokens, pre_mix_gain, w_gate_in, w_input, mix_kernel, w_recur, w_inject, decay_param,
    w_mix_out, post_mix_gain, pre_ffn_gain, w_up_gate, w_up_value, gate_kernel, value_kernel,
    w_down, post_ffn_gain,
):
    ffn_own = jnp.concatenate([w_up_gate, w_up_value, w_down.T], axis=1)
    ffn_all = lax.all_gather(ffn_own, FS, axis=0, tiled=True)

    gains = jnp.stack([pre_mix_gain, post_mix_gain, pre_ffn_gain, post_ffn_gain])
    packed = jnp.concatenate([tokens, jnp.pad(gains, ((0, EXTRA - 4), (0, 0)))], axis=0)
    x_blocks = tp_gathered(packed)
    gate_blocks = ring_gathered(jnp.stack(ring_gathered(w_gate_in, "x", NX)), "z", NZ)
    in_blocks = ring_gathered(jnp.stack(ring_gathered(w_input, "z", NZ)), "x", NX)
    out_blocks = ring_gathered(jnp.stack(ring_gathered(w_mix_out.T, "z", NZ)), "x", NX)
    slope = jax.nn.softplus(-decay_param)[None, :]
    mine, theirs, own_rows, gain_rows = mixer(
        (*x_blocks, *gate_blocks, *in_blocks, *out_blocks, mix_kernel, w_recur[0], w_inject[0], slope)
    )
    mixer_sum = summed_rows(mine, theirs)
    middle = (own_rows.astype(f32) + row_normed(mixer_sum, gain_rows[1:2])).astype(bf16)
    normed_own = row_normed(middle, gain_rows[2:3]).astype(bf16)
    taps = jnp.concatenate([gate_kernel, value_kernel], axis=1)
    mine, theirs = ffn(tp_gathered(normed_own), ffn_all, taps)
    ffn_sum = summed_rows(mine, theirs)
    out_rows = (middle.astype(f32) + row_normed(ffn_sum, gain_rows[3:4])).astype(bf16)
    to_columns = out_rows.reshape(OWN, NTP, PIECE).transpose(1, 0, 2)
    arrived = lax.all_to_all(to_columns, TP, 0, 0, tiled=True).reshape(NY, NC, OWN, PIECE)
    return arrived.transpose(1, 0, 2, 3).reshape(ROWS, PIECE)


def solution(mesh):
    finer = Mesh(mesh.devices.reshape(NZ, NX, NY, NC), ("z", "x", "y", "c"))
    return jax.shard_map(
        shards,
        mesh=finer,
        in_specs=(
            P(FS, TP), P(TP), P(FS, TP), P(FS, TP), P(None, TP), P(TP, None, None),
            P(TP, None, None), P(TP), P(TP, FS), P(TP), P(TP), P(FS, TP), P(FS, TP),
            P(None, TP), P(None, TP), P(TP, FS), P(TP),
        ),
        out_specs=P(FS, TP),
        check_vma=False,
    )
```

```python
import jax
import jax.numpy as jnp
from jax import lax
from jax.experimental import pallas as pl
from jax.experimental.pallas import tpu as pltpu
from jax.sharding import Mesh
from jax.sharding import PartitionSpec as P

D = 2048
FS = ("z", "x")
TP = ("y", "c")
NZ, NX, NY, NC = 8, 4, 4, 2
NTP = NY * NC
ROWS = 512
OWN = ROWS // NTP
PIECE = D // NTP
EXTRA = 16
UNITS = 704
norm_eps = 1e-06
gate_power = 8.0
bf16, f32 = jnp.bfloat16, jnp.float32


def spread(value, axis, n):
    pairs = [(2 * i, 2 * ((i + 1) % n)) for i in range(n)]
    pairs += [(2 * i + 1, 2 * ((i - 1) % n) + 1) for i in range(n)]
    return lax.ppermute(value, (axis, "c"), pairs)


def swapped(value):
    return lax.ppermute(value, "c", [(0, 1), (1, 0)])


def ring_pieces(pack, axis, n):
    p = [pack]
    for _ in range(1, n // 2):
        p.append(spread(p[-1], axis, n))
    return p, spread(p[-1][0], axis, n)


def full_ring(block, axis, n):
    other = swapped(block)
    p, far = ring_pieces(jnp.stack([block, other]), axis, n)
    q = [None] + [swapped(v) for v in p[1:]]
    far_other = swapped(far)
    up, down = range(1, n // 2), range(n // 2 - 1, 0, -1)
    own_row = [block] + [p[k][0] for k in up] + [far] + [q[k][1] for k in down]
    other_row = [other] + [q[k][0] for k in up] + [far_other] + [p[k][1] for k in down]
    return jnp.stack([jnp.stack(own_row), jnp.stack(other_row)])


def own_ring(pack, axis, n):
    p, far = ring_pieces(pack, axis, n)
    return p + [far] + [swapped(p[k][1]) for k in range(n // 2 - 1, 0, -1)]


def rows_ring(pack):
    p, far = ring_pieces(pack, "y", NY)
    return [p[0], p[1], far, swapped(p[1]), swapped(far)]


Y_ORDER = (
    (0, 0, 0, 0), (0, 1, 0, 1), (1, 0, 1, 0), (1, 1, 1, 1),
    (2, None, 2, 0), (4, None, 2, 1), (3, 1, 3, 0), (3, 0, 3, 1),
)


def reduced_rows(give_far, give_next, keep_far, keep_next, home):
    far = (keep_far.astype(f32) + swapped(give_far).astype(f32)).astype(bf16)
    far = spread(far, "y", NY)
    follow = keep_next.astype(f32) + swapped(give_next).astype(f32)
    follow = jnp.concatenate([follow[:OWN] + far.astype(f32), follow[OWN:]], axis=0).astype(bf16)
    return (home.astype(f32) + spread(follow, "y", NY).astype(f32)).astype(bf16)


def row_normed(values, row_gain):
    widened = values.astype(f32)
    factor = lax.rsqrt(jnp.sum(widened * widened, axis=1, keepdims=True) / D + norm_eps)
    return widened * factor * row_gain.astype(f32)


def gelu(v):
    return 0.5 * v * (1.0 + jnp.tanh(0.7978845608028654 * (v + 0.044715 * v * v * v)))


def one_less_exp(u):
    s = 1.0 + u * (1.0 / 8.0)
    for k in range(7, 1, -1):
        s = 1.0 + u * (1.0 / k) * s
    return jnp.where(u > -0.5, -u * s, 1.0 - jnp.exp(u))


def shifted_down(values, by, rows):
    return jnp.where(rows >= by, pltpu.roll(values, by, 0), 0.0)


def stretch(index, size):
    return pl.ds(pl.multiple_of(index * size, size), size)


def upstream(axis, n, k):
    sign = 1 - 2 * lax.axis_index("c")
    return lax.rem(lax.axis_index(axis) + n - k * sign, n)


def core(rel):
    return lax.axis_index("c") if rel == 0 else 1 - lax.axis_index("c")


def own_part(refs, k, n):
    return refs[k].at[0] if k < n // 2 else refs[k]


def dot_nt(a, b):
    return lax.dot_general(a, b, (((1,), (1,)), ((), ())), preferred_element_type=f32)


def projected(hid_ref, turned_ref, wout_ref, outs):
    my = lax.axis_index("y")
    sign = 1 - 2 * lax.axis_index("c")
    ahead, behind = lax.rem(my + NY + sign, NY), lax.rem(my + NY - sign, NY)
    across = lax.rem(my + 2, NY)
    order = [
        (across, 1), (behind, 1), (behind, 0), (across, 0), (ahead, 0), (ahead, 1), (my, 0), (my, 1),
    ]
    for i, (chip, rel) in enumerate(order):
        turned_ref[i * OWN : (i + 1) * OWN, :] = hid_ref[stretch(chip * NC + core(rel), OWN), :]

    def columns(k, _):
        at = stretch(k, PIECE)
        part = dot_nt(turned_ref[...], wout_ref[at, :]).astype(bf16)
        first = 0
        for ref in outs:
            ref[:, at] = part[first : first + ref.shape[0], :]
            first += ref.shape[0]
        return 0

    lax.fori_loop(0, NTP, columns, 0)


def mixer_kernel(*refs):
    x_refs, gate_refs, in_refs, out_refs = refs[0:5], refs[5:13], refs[13:17], refs[17:21]
    taps_ref, recur_ref, inject_ref, slope_ref = refs[21:25]
    outs, own_ref, gain_ref = refs[25:30], refs[30], refs[31]
    win_ref, wout_ref, keep_ref, drive_ref, hid_ref, turned_ref, sems = refs[32:]
    copies = []
    for kz in range(NZ):
        for kx in range(NX):
            rows = stretch(upstream("z", NZ, kz) * NX + upstream("x", NX, kx), 64)
            for source, target in (
                (own_part(gate_refs, kz, NZ).at[kx], win_ref.at[rows, 0:PIECE]),
                (own_part(in_refs, kx, NX).at[kz], win_ref.at[rows, PIECE : 2 * PIECE]),
                (own_part(out_refs, kx, NX).at[kz], wout_ref.at[rows, :]),
            ):
                copies.append(pltpu.make_async_copy(source, target, sems.at[len(copies)]))
    for copy in copies:
        copy.start()
    xs = []
    for operand, entry, ky, rel in Y_ORDER:
        ref = x_refs[operand] if entry is None else x_refs[operand].at[entry]
        xs.append((ref, upstream("y", NY, ky) * NC + core(rel)))
    squares = jnp.zeros((ROWS, 1), f32)
    for ref, column in xs:
        v = ref[0:ROWS, :].astype(f32)
        squares = squares + jnp.sum(v * v, axis=1, keepdims=True)
        at = stretch(column, PIECE)
        for rel in (0, 1):
            own_ref[rel * OWN : (rel + 1) * OWN, at] = ref[
                stretch(lax.axis_index("y") * NC + core(rel), OWN), :
            ]
        gain_ref[:, at] = ref[ROWS : ROWS + 8, :]
    factor = lax.rsqrt(squares / D + norm_eps)
    for copy in copies:
        copy.wait()
    both = jnp.zeros((ROWS, 2 * PIECE), f32)
    for ref, column in xs:
        gain = ref[ROWS : ROWS + 1, :].astype(f32)
        v = (ref[0:ROWS, :].astype(f32) * factor * gain).astype(bf16)
        both = both + jnp.dot(v, win_ref[stretch(column, PIECE), :], preferred_element_type=f32)
    gate_rows = both[:, 0:PIECE].astype(bf16)
    input_rows = both[:, PIECE:].astype(bf16).astype(f32)
    rows = lax.broadcasted_iota(jnp.int32, (ROWS, PIECE), 0)
    taps = taps_ref[...].astype(f32)
    smoothed = input_rows * taps[3:4, :]
    for back in (1, 2, 3):
        smoothed = smoothed + shifted_down(input_rows, back, rows) * taps[3 - back : 4 - back, :]
    smoothed = smoothed.astype(bf16)
    recur = jax.nn.sigmoid(jnp.dot(smoothed, recur_ref[...], preferred_element_type=f32))
    inject = jax.nn.sigmoid(jnp.dot(smoothed, inject_ref[...], preferred_element_type=f32))
    log_retain = -gate_power * recur * slope_ref[...]
    keep = jnp.exp(log_retain)
    drive = jnp.sqrt(one_less_exp(2.0 * log_retain)) * inject * smoothed.astype(f32)
    within = rows % 8
    for by in (1, 2, 4):
        ok = within >= by
        drive = jnp.where(ok, keep * pltpu.roll(drive, by, 0), 0.0) + drive
        keep = jnp.where(ok, pltpu.roll(keep, by, 0), 1.0) * keep
    keep_ref[...] = keep
    drive_ref[...] = drive

    def tile(i, carry):
        at = pl.ds(pl.multiple_of(i * 8, 8), 8)
        state = keep_ref[at, :] * carry + drive_ref[at, :]
        drive_ref[at, :] = state
        return state[7:8, :]

    lax.fori_loop(0, ROWS // 8, tile, jnp.zeros((1, PIECE), f32), unroll=8)
    hid_ref[...] = (gelu(gate_rows.astype(f32)) * drive_ref[...]).astype(bf16)
    projected(hid_ref, turned_ref, wout_ref, outs)


VMEM = pl.BlockSpec(memory_space=pltpu.VMEM)
PARTS = tuple(jax.ShapeDtypeStruct((n * OWN, D), bf16) for n in (1, 2, 1, 2, 2))


def mixer(operands):
    return pl.pallas_call(
        mixer_kernel,
        out_shape=(
            *PARTS, jax.ShapeDtypeStruct((2 * OWN, D), bf16), jax.ShapeDtypeStruct((8, D), bf16),
        ),
        in_specs=[VMEM] * len(operands),
        out_specs=(VMEM,) * 7,
        scratch_shapes=[
            pltpu.VMEM((D, 512), bf16),
            pltpu.VMEM((D, PIECE), bf16),
            pltpu.VMEM((ROWS, PIECE), f32),
            pltpu.VMEM((ROWS, PIECE), f32),
            pltpu.VMEM((ROWS, PIECE), bf16),
            pltpu.VMEM((ROWS, PIECE), bf16),
            pltpu.SemaphoreType.DMA((3 * NZ * NX,)),
        ],
        compiler_params=pltpu.CompilerParams(vmem_limit_bytes=40 * 1024 * 1024),
        cost_estimate=pl.CostEstimate(
            flops=2 * ROWS * D * 768 + 4 * ROWS * PIECE * PIECE,
            bytes_accessed=8 * 1024 * 1024, transcendentals=ROWS * PIECE * 6,
        ),
        name="mixer",
    )(*operands)


UP_CUT = 256
UP_CUTS = 6
TOP = 16


def ffn_kernel(*refs):
    n_refs = refs[0:5]
    w_ref, taps_ref = refs[5:7]
    outs = refs[7:12]
    n_all, up_w, down_w, up_ref, act_ref, turned_ref, sems = refs[12:]

    def cut(i, size):
        at = pl.ds(pl.multiple_of(i * UP_CUT, UP_CUT), size)
        return pltpu.make_async_copy(w_ref.at[:, at], up_w.at[:, at], sems.at[i])

    for i in range(UP_CUTS):
        cut(i, UP_CUT if i < UP_CUTS - 1 else 128).start()
    down = pltpu.make_async_copy(w_ref.at[:, pl.ds(2 * UNITS, UNITS)], down_w, sems.at[UP_CUTS])
    down.start()
    for operand, entry, ky, rel in Y_ORDER:
        ref = n_refs[operand] if entry is None else n_refs[operand].at[entry]
        n_all[stretch(upstream("y", NY, ky) * NC + core(rel), OWN), :] = ref[...]
    up_ref[0:TOP, :] = jnp.zeros((TOP, 2 * UNITS), bf16)

    def up(i, _):
        cut(i, UP_CUT).wait()
        at = stretch(i, UP_CUT)
        up_ref[TOP:, at] = jnp.dot(
            n_all[...], up_w[:, at], preferred_element_type=f32
        ).astype(bf16)
        return 0

    lax.fori_loop(0, UP_CUTS - 1, up, 0)
    cut(UP_CUTS - 1, 128).wait()
    last = slice((UP_CUTS - 1) * UP_CUT, 2 * UNITS)
    up_ref[TOP:, last] = jnp.dot(n_all[...], up_w[:, last], preferred_element_type=f32).astype(bf16)
    taps = taps_ref[...].astype(f32)

    def smooth(i, _):
        at = pl.multiple_of(i * 64, 64)
        v = up_ref[pl.ds(at, 64 + TOP), :].astype(f32)
        conv = v[TOP:] * taps[2:3, :]
        for back in (1, 2):
            conv = conv + pltpu.roll(v, back, 0)[TOP:] * taps[2 - back : 3 - back, :]
        act_ref[pl.ds(at, 64), :] = (gelu(conv[:, 0:UNITS]) * conv[:, UNITS:]).astype(bf16)
        return 0

    lax.fori_loop(0, ROWS // 64, smooth, 0)
    down.wait()
    projected(act_ref, turned_ref, down_w, outs)


def ffn(blocks, w_all, taps):
    return pl.pallas_call(
        ffn_kernel,
        out_shape=PARTS,
        in_specs=[VMEM] * 5 + [pl.BlockSpec(memory_space=pl.ANY), VMEM],
        out_specs=(VMEM,) * 5,
        scratch_shapes=[
            pltpu.VMEM((ROWS, D), bf16),
            pltpu.VMEM((D, 2 * UNITS), bf16),
            pltpu.VMEM((D, UNITS), bf16),
            pltpu.VMEM((ROWS + TOP, 2 * UNITS), bf16),
            pltpu.VMEM((ROWS, UNITS), bf16),
            pltpu.VMEM((ROWS, UNITS), bf16),
            pltpu.SemaphoreType.DMA((UP_CUTS + 1,)),
        ],
        compiler_params=pltpu.CompilerParams(vmem_limit_bytes=44 * 1024 * 1024),
        cost_estimate=pl.CostEstimate(
            flops=2 * ROWS * D * 3 * UNITS, bytes_accessed=13 * 1024 * 1024,
            transcendentals=ROWS * UNITS,
        ),
        name="ffn",
    )(*blocks, w_all, taps)


def shards(
    tokens, pre_mix_gain, w_gate_in, w_input, mix_kernel, w_recur, w_inject, decay_param,
    w_mix_out, post_mix_gain, pre_ffn_gain, w_up_gate, w_up_value, gate_kernel, value_kernel,
    w_down, post_ffn_gain,
):
    ffn_own = jnp.concatenate([w_up_gate, w_up_value, w_down.T], axis=1)
    ffn_all = lax.all_gather(ffn_own, FS, axis=0, tiled=True)

    gains = jnp.stack([pre_mix_gain, post_mix_gain, pre_ffn_gain, post_ffn_gain])
    packed = jnp.concatenate([tokens, jnp.pad(gains, ((0, EXTRA - 4), (0, 0)))], axis=0)
    x_blocks = rows_ring(jnp.stack([packed, swapped(packed)]))
    gate_blocks = own_ring(full_ring(w_gate_in, "x", NX), "z", NZ)
    in_blocks = own_ring(full_ring(w_input, "z", NZ), "x", NX)
    out_blocks = own_ring(full_ring(w_mix_out.T, "z", NZ), "x", NX)
    slope = jax.nn.softplus(-decay_param)[None, :]
    *parts, own_rows, gain_rows = mixer(
        (*x_blocks, *gate_blocks, *in_blocks, *out_blocks, mix_kernel, w_recur[0], w_inject[0], slope)
    )
    part = reduced_rows(*parts)
    turned = swapped(jnp.concatenate([part[OWN:], part[:OWN]], axis=0))
    mixer_sum = part.astype(f32) + turned.astype(f32)
    middle = (own_rows.astype(f32) + row_normed(mixer_sum, gain_rows[1:2])).astype(bf16)
    normed = row_normed(middle, gain_rows[2:3]).astype(bf16)
    taps = jnp.concatenate([gate_kernel, value_kernel], axis=1)
    parts = ffn(rows_ring(normed.reshape(2, OWN, D)), ffn_all, taps)
    part = reduced_rows(*parts)
    ffn_sum = part[:OWN].astype(f32) + swapped(part[OWN:]).astype(f32)
    out_rows = (middle[:OWN].astype(f32) + row_normed(ffn_sum, gain_rows[3:4])).astype(bf16)
    to_columns = out_rows.reshape(OWN, NTP, PIECE).transpose(1, 0, 2)
    return lax.all_to_all(to_columns, TP, 0, 0, tiled=True).reshape(ROWS, PIECE)


def solution(mesh):
    finer = Mesh(mesh.devices.reshape(NZ, NX, NY, NC), ("z", "x", "y", "c"))
    return jax.shard_map(
        shards,
        mesh=finer,
        in_specs=(
            P(FS, TP), P(TP), P(FS, TP), P(FS, TP), P(None, TP), P(TP, None, None),
            P(TP, None, None), P(TP), P(TP, FS), P(TP), P(TP), P(FS, TP), P(FS, TP),
            P(None, TP), P(None, TP), P(TP, FS), P(TP),
        ),
        out_specs=P(FS, TP),
        check_vma=False,
    )
```

```python
import jax
import jax.numpy as jnp
from jax import lax
from jax.experimental import pallas as pl
from jax.experimental.pallas import tpu as pltpu
from jax.sharding import Mesh
from jax.sharding import PartitionSpec as P

D = 2048
FS = ("z", "x")
TP = ("y", "c")
NZ, NX, NY, NC = 8, 4, 4, 2
NTP = NY * NC
ROWS = 512
OWN = ROWS // NTP
PIECE = D // NTP
EXTRA = 16
UNITS = 704
norm_eps = 1e-06
gate_power = 8.0
bf16, f32 = jnp.bfloat16, jnp.float32


def moved(value, axis, n, by):
    return lax.ppermute(value, axis, [(i, (i + by) % n) for i in range(n)])


def ring_gathered(block, axis, n):
    got = [block] + [None] * (n - 1)
    ahead = back = block
    for s in range(1, n // 2):
        ahead = moved(ahead, axis, n, 1)
        back = moved(back, axis, n, -1)
        got[s], got[n - s] = ahead, back
    half = block.shape[0] // 2
    first = moved(ahead[:half], axis, n, 1)
    second = moved(back[half:], axis, n, -1)
    got[n // 2] = jnp.concatenate([first, second], axis=0)
    return got


def swapped(value):
    return lax.ppermute(value, "c", [(0, 1), (1, 0)])


def tp_gathered(block):
    near = ring_gathered(block, "y", NY)
    return [v for b in near for v in (b, swapped(b))]


def summed_rows(mine, theirs):
    half = OWN // 2
    far = mine[2].astype(f32) + swapped(theirs[2]).astype(f32)
    far = far.astype(bf16)
    first = moved(far[:half], "y", NY, 1)
    second = moved(far[half:], "y", NY, -1)
    one = mine[1].astype(f32) + swapped(theirs[1]).astype(f32)
    back = mine[3].astype(f32) + swapped(theirs[3]).astype(f32)
    own = mine[0].astype(f32) + swapped(theirs[0]).astype(f32)
    one = jnp.concatenate([one[:half] + first.astype(f32), one[half:]], axis=0).astype(bf16)
    back = jnp.concatenate([back[:half], back[half:] + second.astype(f32)], axis=0).astype(bf16)
    return own + moved(one, "y", NY, 1).astype(f32) + moved(back, "y", NY, -1).astype(f32)


def row_normed(values, row_gain):
    widened = values.astype(f32)
    factor = lax.rsqrt(jnp.sum(widened * widened, axis=1, keepdims=True) / D + norm_eps)
    return widened * factor * row_gain.astype(f32)


def gelu(v):
    return 0.5 * v * (1.0 + jnp.tanh(0.7978845608028654 * (v + 0.044715 * v * v * v)))


def one_less_exp(u):
    s = 1.0 + u * (1.0 / 8.0)
    for k in range(7, 1, -1):
        s = 1.0 + u * (1.0 / k) * s
    return jnp.where(u > -0.5, -u * s, 1.0 - jnp.exp(u))


def shifted_down(values, by, rows):
    return jnp.where(rows >= by, pltpu.roll(values, by, 0), 0.0)


def stretch(index, size):
    return pl.ds(pl.multiple_of(index * size, size), size)


def behind(me, by, n):
    return lax.rem(me + (n - by), n)


def dot_nt(a, b):
    return lax.dot_general(a, b, (((1,), (1,)), ((), ())), preferred_element_type=f32)


def sent_to_all(shard, axis, devices):
    return lax.all_to_all(
        jnp.broadcast_to(shard[None], (devices, *shard.shape)), axis, 0, 0, tiled=True
    )


def fs_gathered(block):
    along_z = sent_to_all(block, "z", NZ).reshape(NZ, *block.shape)
    return ring_gathered(along_z, "x", NX)


def column_of(k):
    mc = lax.axis_index("c")
    return behind(lax.axis_index("y"), k // 2, NY) * NC + (mc if k % 2 == 0 else 1 - mc)


def mixer_kernel(*refs):
    x_refs, w_refs = refs[0:8], refs[8:12]
    taps_ref, recur_ref, inject_ref, slope_ref = refs[12:16]
    mine_ref, theirs_ref, own_ref, gain_ref = refs[16:20]
    win_ref, wout_ref, keep_ref, drive_ref, hid_ref, sems = refs[20:]
    mx, my, mc = lax.axis_index("x"), lax.axis_index("y"), lax.axis_index("c")
    ins, outs = [], []
    for k in range(NX):
        at = behind(mx, k, NX)
        ins.append(pltpu.make_async_copy(
            w_refs[k].at[:, :, pl.ds(0, 512)], win_ref.at[:, at], sems.at[k]
        ))
        outs.append(pltpu.make_async_copy(
            w_refs[k].at[:, :, pl.ds(512, PIECE)], wout_ref.at[:, at], sems.at[NX + k]
        ))
    for copy in ins + outs:
        copy.start()
    first_own = pl.multiple_of(mc * 256 + my * OWN, OWN)
    squares = jnp.zeros((ROWS, 1), f32)
    for k in range(NTP):
        v = x_refs[k][0:ROWS, :].astype(f32)
        squares = squares + jnp.sum(v * v, axis=1, keepdims=True)
        at = stretch(column_of(k), PIECE)
        own_ref[:, at] = x_refs[k][pl.ds(first_own, OWN), :]
        gain_ref[:, at] = x_refs[k][ROWS : ROWS + 8, :]
    factor = lax.rsqrt(squares / D + norm_eps)
    for copy in ins:
        copy.wait()
    both = jnp.zeros((ROWS, 2 * PIECE), f32)
    for k in range(NTP):
        gain = x_refs[k][ROWS : ROWS + 1, :].astype(f32)
        v = (x_refs[k][0:ROWS, :].astype(f32) * factor * gain).astype(bf16)
        w = win_ref[column_of(k)].reshape(PIECE, 512)
        both = both + jnp.dot(v, w, preferred_element_type=f32)
    gate_rows = both[:, 0:PIECE].astype(bf16)
    input_rows = both[:, PIECE:].astype(bf16).astype(f32)
    rows = lax.broadcasted_iota(jnp.int32, (ROWS, PIECE), 0)
    taps = taps_ref[...].astype(f32)
    smoothed = input_rows * taps[3:4, :]
    for back in (1, 2, 3):
        smoothed = smoothed + shifted_down(input_rows, back, rows) * taps[3 - back : 4 - back, :]
    smoothed = smoothed.astype(bf16)
    recur = jax.nn.sigmoid(jnp.dot(smoothed, recur_ref[...], preferred_element_type=f32))
    inject = jax.nn.sigmoid(jnp.dot(smoothed, inject_ref[...], preferred_element_type=f32))
    log_retain = -gate_power * recur * slope_ref[...]
    keep = jnp.exp(log_retain)
    drive = jnp.sqrt(one_less_exp(2.0 * log_retain)) * inject * smoothed.astype(f32)
    within = rows % 8
    for by in (1, 2, 4):
        ok = within >= by
        drive = jnp.where(ok, keep * pltpu.roll(drive, by, 0), 0.0) + drive
        keep = jnp.where(ok, pltpu.roll(keep, by, 0), 1.0) * keep
    keep_ref[...] = keep
    drive_ref[...] = drive

    def tile(i, carry):
        at = pl.ds(pl.multiple_of(i * 8, 8), 8)
        state = keep_ref[at, :] * carry + drive_ref[at, :]
        drive_ref[at, :] = state
        return state[7:8, :]

    lax.fori_loop(0, ROWS // 8, tile, jnp.zeros((1, PIECE), f32), unroll=8)
    hid_ref[...] = (gelu(gate_rows.astype(f32)) * drive_ref[...]).astype(bf16)
    for copy in outs:
        copy.wait()
    projected(hid_ref, wout_ref, mine_ref, theirs_ref)


def projected(hid_ref, wout_ref, mine_ref, theirs_ref):
    my, mc = lax.axis_index("y"), lax.axis_index("c")

    def columns(k, _):
        w = wout_ref[k].reshape(PIECE, -1)
        at = stretch(k, PIECE)
        for ref, half in ((theirs_ref, 1 - mc), (mine_ref, mc)):
            part = dot_nt(hid_ref[stretch(half, 256), :], w).astype(bf16)
            for y in range(NY):
                ref[lax.rem(y + NY - my, NY), :, at] = part[y * OWN : (y + 1) * OWN, :]
        return 0

    lax.fori_loop(0, NZ, columns, 0)


VMEM = pl.BlockSpec(memory_space=pltpu.VMEM)
BY_ROWS = jax.ShapeDtypeStruct((NY, OWN, D), bf16)


def mixer(operands):
    return pl.pallas_call(
        mixer_kernel,
        out_shape=(
            BY_ROWS, BY_ROWS,
            jax.ShapeDtypeStruct((OWN, D), bf16), jax.ShapeDtypeStruct((8, D), bf16),
        ),
        in_specs=[VMEM] * len(operands),
        out_specs=(VMEM,) * 4,
        scratch_shapes=[
            pltpu.VMEM((NZ, NX, 64, 512), bf16),
            pltpu.VMEM((NZ, NX, 64, PIECE), bf16),
            pltpu.VMEM((ROWS, PIECE), f32),
            pltpu.VMEM((ROWS, PIECE), f32),
            pltpu.VMEM((ROWS, PIECE), bf16),
            pltpu.SemaphoreType.DMA((2 * NX,)),
        ],
        compiler_params=pltpu.CompilerParams(vmem_limit_bytes=40 * 1024 * 1024),
        cost_estimate=pl.CostEstimate(
            flops=2 * ROWS * D * 768 + 4 * ROWS * PIECE * PIECE,
            bytes_accessed=8 * 1024 * 1024, transcendentals=ROWS * PIECE * 6,
        ),
        name="mixer",
    )(*operands)


UP_CUT = 256
UP_CUTS = 6
TOP = 16


def ffn_kernel(*refs):
    n_refs, d_refs = refs[0:8], refs[8:12]
    w_ref, taps_ref = refs[12:14]
    mine_ref, theirs_ref = refs[14:16]
    n_all, up_w, down_w, up_ref, act_ref, sems = refs[16:]
    mx, my, mc = lax.axis_index("x"), lax.axis_index("y"), lax.axis_index("c")

    def cut(i, size):
        at = pl.ds(pl.multiple_of(i * UP_CUT, UP_CUT), size)
        return pltpu.make_async_copy(w_ref.at[:, at], up_w.at[:, at], sems.at[i])

    for i in range(UP_CUTS):
        cut(i, UP_CUT if i < UP_CUTS - 1 else 128).start()
    downs = [
        pltpu.make_async_copy(d_refs[k], down_w.at[:, behind(mx, k, NX)], sems.at[UP_CUTS + k])
        for k in range(NX)
    ]
    for copy in downs:
        copy.start()
    for k in range(NTP):
        half = mc if k % 2 == 0 else 1 - mc
        n_all[stretch(half * NY + behind(my, k // 2, NY), OWN), :] = n_refs[k][...]
    up_ref[0:TOP, :] = jnp.zeros((TOP, 2 * UNITS), bf16)

    def up(i, _):
        cut(i, UP_CUT).wait()
        at = stretch(i, UP_CUT)
        up_ref[TOP:, at] = jnp.dot(
            n_all[...], up_w[:, at], preferred_element_type=f32
        ).astype(bf16)
        return 0

    lax.fori_loop(0, UP_CUTS - 1, up, 0)
    cut(UP_CUTS - 1, 128).wait()
    last = slice((UP_CUTS - 1) * UP_CUT, 2 * UNITS)
    up_ref[TOP:, last] = jnp.dot(n_all[...], up_w[:, last], preferred_element_type=f32).astype(bf16)
    taps = taps_ref[...].astype(f32)

    def smooth(i, _):
        at = pl.multiple_of(i * 64, 64)
        v = up_ref[pl.ds(at, 64 + TOP), :].astype(f32)
        conv = v[TOP:] * taps[2:3, :]
        for back in (1, 2):
            conv = conv + pltpu.roll(v, back, 0)[TOP:] * taps[2 - back : 3 - back, :]
        act_ref[pl.ds(at, 64), :] = (gelu(conv[:, 0:UNITS]) * conv[:, UNITS:]).astype(bf16)
        return 0

    lax.fori_loop(0, ROWS // 64, smooth, 0)
    for copy in downs:
        copy.wait()
    projected(act_ref, down_w, mine_ref, theirs_ref)


def ffn(blocks, down_blocks, w_all, taps):
    return pl.pallas_call(
        ffn_kernel,
        out_shape=(BY_ROWS, BY_ROWS),
        in_specs=[VMEM] * 8 + [pl.BlockSpec(memory_space=pl.ANY)] * 5 + [VMEM],
        out_specs=(VMEM, VMEM),
        scratch_shapes=[
            pltpu.VMEM((ROWS, D), bf16),
            pltpu.VMEM((D, 2 * UNITS), bf16),
            pltpu.VMEM((NZ, NX, 64, UNITS), bf16),
            pltpu.VMEM((ROWS + TOP, 2 * UNITS), bf16),
            pltpu.VMEM((ROWS, UNITS), bf16),
            pltpu.SemaphoreType.DMA((UP_CUTS + NX,)),
        ],
        compiler_params=pltpu.CompilerParams(vmem_limit_bytes=44 * 1024 * 1024),
        cost_estimate=pl.CostEstimate(
            flops=2 * ROWS * D * 3 * UNITS, bytes_accessed=13 * 1024 * 1024,
            transcendentals=ROWS * UNITS,
        ),
        name="ffn",
    )(*blocks, *down_blocks, w_all, taps)


def shards(
    tokens, pre_mix_gain, w_gate_in, w_input, mix_kernel, w_recur, w_inject, decay_param,
    w_mix_out, post_mix_gain, pre_ffn_gain, w_up_gate, w_up_value, gate_kernel, value_kernel,
    w_down, post_ffn_gain,
):
    up_all = lax.all_gather(
        jnp.concatenate([w_up_gate, w_up_value], axis=1), FS, axis=0, tiled=True
    )
    gains = jnp.stack([pre_mix_gain, post_mix_gain, pre_ffn_gain, post_ffn_gain])
    packed = jnp.concatenate([tokens, jnp.pad(gains, ((0, EXTRA - 4), (0, 0)))], axis=0)
    mix_blocks = fs_gathered(jnp.concatenate([w_gate_in, w_input, w_mix_out.T], axis=1))
    x_blocks = tp_gathered(packed)
    down_blocks = fs_gathered(w_down.T)
    slope = jax.nn.softplus(-decay_param)[None, :]
    mine, theirs, own_rows, gain_rows = mixer(
        (*x_blocks, *mix_blocks, mix_kernel, w_recur[0], w_inject[0], slope)
    )
    mixer_sum = summed_rows(mine, theirs)
    middle = (own_rows.astype(f32) + row_normed(mixer_sum, gain_rows[1:2])).astype(bf16)
    normed_own = row_normed(middle, gain_rows[2:3]).astype(bf16)
    taps = jnp.concatenate([gate_kernel, value_kernel], axis=1)
    mine, theirs = ffn(tp_gathered(normed_own), down_blocks, up_all, taps)
    ffn_sum = summed_rows(mine, theirs)
    out_rows = (middle.astype(f32) + row_normed(ffn_sum, gain_rows[3:4])).astype(bf16)
    to_columns = out_rows.reshape(OWN, NTP, PIECE).transpose(1, 0, 2)
    arrived = lax.all_to_all(to_columns, TP, 0, 0, tiled=True).reshape(NY, NC, OWN, PIECE)
    return arrived.transpose(1, 0, 2, 3).reshape(ROWS, PIECE)


def solution(mesh):
    finer = Mesh(mesh.devices.reshape(NZ, NX, NY, NC), ("z", "x", "y", "c"))
    return jax.shard_map(
        shards,
        mesh=finer,
        in_specs=(
            P(FS, TP), P(TP), P(FS, TP), P(FS, TP), P(None, TP), P(TP, None, None),
            P(TP, None, None), P(TP), P(TP, FS), P(TP), P(TP), P(FS, TP), P(FS, TP),
            P(None, TP), P(None, TP), P(TP, FS), P(TP),
        ),
        out_specs=P(FS, TP),
        check_vma=False,
    )
```

```python
import jax
import jax.numpy as jnp
from jax import lax
from jax.experimental import pallas as pl
from jax.experimental.pallas import tpu as pltpu
from jax.sharding import Mesh
from jax.sharding import PartitionSpec as P

D = 2048
FS = ("z", "x")
TP = ("y", "c")
NZ, NX, NY, NC = 8, 4, 4, 2
NTP = NY * NC
ROWS = 512
OWN = ROWS // NTP
PIECE = D // NTP
EXTRA = 16
UNITS = 704
norm_eps = 1e-06
gate_power = 8.0
bf16, f32 = jnp.bfloat16, jnp.float32


def moved(value, axis, n, by):
    return lax.ppermute(value, axis, [(i, (i + by) % n) for i in range(n)])


def ring_gathered(block, axis, n):
    got = [block] + [None] * (n - 1)
    ahead = back = block
    for s in range(1, n // 2):
        ahead = moved(ahead, axis, n, 1)
        back = moved(back, axis, n, -1)
        got[s], got[n - s] = ahead, back
    half = block.shape[0] // 2
    first = moved(ahead[:half], axis, n, 1)
    second = moved(back[half:], axis, n, -1)
    got[n // 2] = jnp.concatenate([first, second], axis=0)
    return got


def swapped(value):
    return lax.ppermute(value, "c", [(0, 1), (1, 0)])


def tp_gathered(block):
    near = ring_gathered(block, "y", NY)
    return [v for b in near for v in (b, swapped(b))]


def summed_rows(mine, theirs):
    half = OWN // 2
    far = mine[2].astype(f32) + swapped(theirs[2]).astype(f32)
    far = far.astype(bf16)
    first = moved(far[:half], "y", NY, 1)
    second = moved(far[half:], "y", NY, -1)
    one = mine[1].astype(f32) + swapped(theirs[1]).astype(f32)
    back = mine[3].astype(f32) + swapped(theirs[3]).astype(f32)
    own = mine[0].astype(f32) + swapped(theirs[0]).astype(f32)
    one = jnp.concatenate([one[:half] + first.astype(f32), one[half:]], axis=0).astype(bf16)
    back = jnp.concatenate([back[:half], back[half:] + second.astype(f32)], axis=0).astype(bf16)
    return own + moved(one, "y", NY, 1).astype(f32) + moved(back, "y", NY, -1).astype(f32)


def row_normed(values, row_gain):
    widened = values.astype(f32)
    factor = lax.rsqrt(jnp.sum(widened * widened, axis=1, keepdims=True) / D + norm_eps)
    return widened * factor * row_gain.astype(f32)


def gelu(v):
    return 0.5 * v * (1.0 + jnp.tanh(0.7978845608028654 * (v + 0.044715 * v * v * v)))


def one_less_exp(u):
    s = 1.0 + u * (1.0 / 8.0)
    for k in range(7, 1, -1):
        s = 1.0 + u * (1.0 / k) * s
    return jnp.where(u > -0.5, -u * s, 1.0 - jnp.exp(u))


def shifted_down(values, by, rows):
    return jnp.where(rows >= by, pltpu.roll(values, by, 0), 0.0)


def stretch(index, size):
    return pl.ds(pl.multiple_of(index * size, size), size)


def behind(me, by, n):
    return lax.rem(me + (n - by), n)


def dot_nt(a, b):
    return lax.dot_general(a, b, (((1,), (1,)), ((), ())), preferred_element_type=f32)


def rings(block, first, n_first, second, n_second):
    return ring_gathered(jnp.stack(ring_gathered(block, first, n_first)), second, n_second)


def column_of(k):
    mc = lax.axis_index("c")
    return behind(lax.axis_index("y"), k // 2, NY) * NC + (mc if k % 2 == 0 else 1 - mc)


def mixer_kernel(*refs):
    x_refs, w_refs = refs[0:8], refs[8:12]
    taps_ref, recur_ref, inject_ref, slope_ref = refs[12:16]
    mine_ref, theirs_ref, own_ref, gain_ref = refs[16:20]
    win_ref, wout_ref, keep_ref, drive_ref, hid_ref = refs[20:]
    mz, mx = lax.axis_index("z"), lax.axis_index("x")
    my, mc = lax.axis_index("y"), lax.axis_index("c")

    def placed(kz, _):
        for kx in range(NX):
            z, x = lax.rem(mz + NZ - kz, NZ), behind(mx, kx, NX)
            win_ref[z, x] = w_refs[kx][kz, :, 0:512]
            wout_ref[z, x] = w_refs[kx][kz, :, 512:]
        return 0

    lax.fori_loop(0, NZ, placed, 0)
    first_own = pl.multiple_of(mc * 256 + my * OWN, OWN)
    squares = jnp.zeros((ROWS, 1), f32)
    for k in range(NTP):
        v = x_refs[k][0:ROWS, :].astype(f32)
        squares = squares + jnp.sum(v * v, axis=1, keepdims=True)
        at = stretch(column_of(k), PIECE)
        own_ref[:, at] = x_refs[k][pl.ds(first_own, OWN), :]
        gain_ref[:, at] = x_refs[k][ROWS : ROWS + 8, :]
    factor = lax.rsqrt(squares / D + norm_eps)
    both = jnp.zeros((ROWS, 2 * PIECE), f32)
    for k in range(NTP):
        gain = x_refs[k][ROWS : ROWS + 1, :].astype(f32)
        v = (x_refs[k][0:ROWS, :].astype(f32) * factor * gain).astype(bf16)
        w = win_ref[column_of(k)].reshape(PIECE, 512)
        both = both + jnp.dot(v, w, preferred_element_type=f32)
    gate_rows = both[:, 0:PIECE].astype(bf16)
    input_rows = both[:, PIECE:].astype(bf16).astype(f32)
    rows = lax.broadcasted_iota(jnp.int32, (ROWS, PIECE), 0)
    taps = taps_ref[...].astype(f32)
    smoothed = input_rows * taps[3:4, :]
    for back in (1, 2, 3):
        smoothed = smoothed + shifted_down(input_rows, back, rows) * taps[3 - back : 4 - back, :]
    smoothed = smoothed.astype(bf16)
    recur = jax.nn.sigmoid(jnp.dot(smoothed, recur_ref[...], preferred_element_type=f32))
    inject = jax.nn.sigmoid(jnp.dot(smoothed, inject_ref[...], preferred_element_type=f32))
    log_retain = -gate_power * recur * slope_ref[...]
    keep = jnp.exp(log_retain)
    drive = jnp.sqrt(one_less_exp(2.0 * log_retain)) * inject * smoothed.astype(f32)
    within = rows % 8
    for by in (1, 2, 4):
        ok = within >= by
        drive = jnp.where(ok, keep * pltpu.roll(drive, by, 0), 0.0) + drive
        keep = jnp.where(ok, pltpu.roll(keep, by, 0), 1.0) * keep
    keep_ref[...] = keep
    drive_ref[...] = drive

    def tile(i, carry):
        at = pl.ds(pl.multiple_of(i * 8, 8), 8)
        state = keep_ref[at, :] * carry + drive_ref[at, :]
        drive_ref[at, :] = state
        return state[7:8, :]

    lax.fori_loop(0, ROWS // 8, tile, jnp.zeros((1, PIECE), f32), unroll=8)
    hid_ref[...] = (gelu(gate_rows.astype(f32)) * drive_ref[...]).astype(bf16)
    projected(hid_ref, wout_ref, mine_ref, theirs_ref)


def projected(hid_ref, wout_ref, mine_ref, theirs_ref):
    my, mc = lax.axis_index("y"), lax.axis_index("c")

    def columns(k, _):
        w = wout_ref[k].reshape(PIECE, -1)
        at = stretch(k, PIECE)
        for ref, half in ((theirs_ref, 1 - mc), (mine_ref, mc)):
            part = dot_nt(hid_ref[stretch(half, 256), :], w).astype(bf16)
            for y in range(NY):
                ref[lax.rem(y + NY - my, NY), :, at] = part[y * OWN : (y + 1) * OWN, :]
        return 0

    lax.fori_loop(0, NZ, columns, 0)


VMEM = pl.BlockSpec(memory_space=pltpu.VMEM)
BY_ROWS = jax.ShapeDtypeStruct((NY, OWN, D), bf16)


def mixer(operands):
    return pl.pallas_call(
        mixer_kernel,
        out_shape=(
            BY_ROWS, BY_ROWS,
            jax.ShapeDtypeStruct((OWN, D), bf16), jax.ShapeDtypeStruct((8, D), bf16),
        ),
        in_specs=[VMEM] * len(operands),
        out_specs=(VMEM,) * 4,
        scratch_shapes=[
            pltpu.VMEM((NZ, NX, 64, 512), bf16),
            pltpu.VMEM((NZ, NX, 64, PIECE), bf16),
            pltpu.VMEM((ROWS, PIECE), f32),
            pltpu.VMEM((ROWS, PIECE), f32),
            pltpu.VMEM((ROWS, PIECE), bf16),
        ],
        compiler_params=pltpu.CompilerParams(vmem_limit_bytes=24 * 1024 * 1024),
        cost_estimate=pl.CostEstimate(
            flops=2 * ROWS * D * 768 + 4 * ROWS * PIECE * PIECE,
            bytes_accessed=8 * 1024 * 1024, transcendentals=ROWS * PIECE * 6,
        ),
        name="mixer",
    )(*operands)


UP_CUT = 256
UP_CUTS = 6
TOP = 16


def ffn_kernel(*refs):
    n_refs, u_refs, d_refs, taps_ref = refs[0:8], refs[8:16], refs[16:20], refs[20]
    mine_ref, theirs_ref = refs[21:23]
    n_all, up_w, down_w, up_ref, act_ref, sems = refs[23:]
    mz, mx = lax.axis_index("z"), lax.axis_index("x")
    my, mc = lax.axis_index("y"), lax.axis_index("c")
    ups, downs = [], []
    for kz in range(NZ):
        for kx in range(NX):
            z, x, i = behind(mz, kz, NZ), behind(mx, kx, NX), len(ups)
            ups.append(pltpu.make_async_copy(u_refs[kz].at[kx], up_w.at[z, x], sems.at[0, i]))
            downs.append(pltpu.make_async_copy(d_refs[kx].at[kz], down_w.at[z, x], sems.at[1, i]))
    for copy in ups + downs:
        copy.start()
    for k in range(NTP):
        half = mc if k % 2 == 0 else 1 - mc
        n_all[stretch(half * NY + behind(my, k // 2, NY), OWN), :] = n_refs[k][...]
    up_ref[0:TOP, :] = jnp.zeros((TOP, 2 * UNITS), bf16)

    for copy in ups:
        copy.wait()

    def up(at):
        w = up_w[:, :, :, at].reshape(D, -1)
        up_ref[TOP:, at] = jnp.dot(n_all[...], w, preferred_element_type=f32).astype(bf16)

    def loop(i, _):
        up(stretch(i, UP_CUT))
        return 0

    lax.fori_loop(0, UP_CUTS - 1, loop, 0)
    up(slice((UP_CUTS - 1) * UP_CUT, 2 * UNITS))
    taps = taps_ref[...].astype(f32)

    def smooth(i, _):
        at = pl.multiple_of(i * 64, 64)
        v = up_ref[pl.ds(at, 64 + TOP), :].astype(f32)
        conv = v[TOP:] * taps[2:3, :]
        for back in (1, 2):
            conv = conv + pltpu.roll(v, back, 0)[TOP:] * taps[2 - back : 3 - back, :]
        act_ref[pl.ds(at, 64), :] = (gelu(conv[:, 0:UNITS]) * conv[:, UNITS:]).astype(bf16)
        return 0

    lax.fori_loop(0, ROWS // 64, smooth, 0)
    for copy in downs:
        copy.wait()
    projected(act_ref, down_w, mine_ref, theirs_ref)


def ffn(operands):
    return pl.pallas_call(
        ffn_kernel,
        out_shape=(BY_ROWS, BY_ROWS),
        in_specs=[VMEM] * 8 + [pl.BlockSpec(memory_space=pl.ANY)] * 12 + [VMEM],
        out_specs=(VMEM, VMEM),
        scratch_shapes=[
            pltpu.VMEM((ROWS, D), bf16),
            pltpu.VMEM((NZ, NX, 64, 2 * UNITS), bf16),
            pltpu.VMEM((NZ, NX, 64, UNITS), bf16),
            pltpu.VMEM((ROWS + TOP, 2 * UNITS), bf16),
            pltpu.VMEM((ROWS, UNITS), bf16),
            pltpu.SemaphoreType.DMA((2, NZ * NX)),
        ],
        compiler_params=pltpu.CompilerParams(vmem_limit_bytes=36 * 1024 * 1024),
        cost_estimate=pl.CostEstimate(
            flops=2 * ROWS * D * 3 * UNITS, bytes_accessed=13 * 1024 * 1024,
            transcendentals=ROWS * UNITS,
        ),
        name="ffn",
    )(*operands)


def shards(
    tokens, pre_mix_gain, w_gate_in, w_input, mix_kernel, w_recur, w_inject, decay_param,
    w_mix_out, post_mix_gain, pre_ffn_gain, w_up_gate, w_up_value, gate_kernel, value_kernel,
    w_down, post_ffn_gain,
):
    gains = jnp.stack([pre_mix_gain, post_mix_gain, pre_ffn_gain, post_ffn_gain])
    packed = jnp.concatenate([tokens, jnp.pad(gains, ((0, EXTRA - 4), (0, 0)))], axis=0)
    mix_own = jnp.concatenate([w_gate_in, w_input, w_mix_out.T], axis=1)
    mix_blocks = rings(mix_own, "z", NZ, "x", NX)
    x_blocks = tp_gathered(packed)
    up_own = jnp.concatenate([w_up_gate, w_up_value], axis=1)
    up_blocks = rings(up_own, "x", NX, "z", NZ)
    down_blocks = rings(w_down.T, "z", NZ, "x", NX)
    slope = jax.nn.softplus(-decay_param)[None, :]
    mine, theirs, own_rows, gain_rows = mixer(
        (*x_blocks, *mix_blocks, mix_kernel, w_recur[0], w_inject[0], slope)
    )
    mixer_sum = summed_rows(mine, theirs)
    middle = (own_rows.astype(f32) + row_normed(mixer_sum, gain_rows[1:2])).astype(bf16)
    normed_own = row_normed(middle, gain_rows[2:3]).astype(bf16)
    taps = jnp.concatenate([gate_kernel, value_kernel], axis=1)
    mine, theirs = ffn((*tp_gathered(normed_own), *up_blocks, *down_blocks, taps))
    ffn_sum = summed_rows(mine, theirs)
    out_rows = (middle.astype(f32) + row_normed(ffn_sum, gain_rows[3:4])).astype(bf16)
    to_columns = out_rows.reshape(OWN, NTP, PIECE).transpose(1, 0, 2)
    arrived = lax.all_to_all(to_columns, TP, 0, 0, tiled=True).reshape(NY, NC, OWN, PIECE)
    return arrived.transpose(1, 0, 2, 3).reshape(ROWS, PIECE)


def solution(mesh):
    finer = Mesh(mesh.devices.reshape(NZ, NX, NY, NC), ("z", "x", "y", "c"))
    return jax.shard_map(
        shards,
        mesh=finer,
        in_specs=(
            P(FS, TP), P(TP), P(FS, TP), P(FS, TP), P(None, TP), P(TP, None, None),
            P(TP, None, None), P(TP), P(TP, FS), P(TP), P(TP), P(FS, TP), P(FS, TP),
            P(None, TP), P(None, TP), P(TP, FS), P(TP),
        ),
        out_specs=P(FS, TP),
        check_vma=False,
    )
```

```python
import jax
import jax.numpy as jnp
from jax import lax
from jax.experimental import pallas as pl
from jax.experimental.pallas import tpu as pltpu
from jax.sharding import Mesh
from jax.sharding import PartitionSpec as P


D = 2048
FS = ("z", "x")
TP = ("y", "c")
NZ, NX, NY, NC = 8, 4, 4, 2
NTP = NY * NC
ROWS = 512
OWN = ROWS // NTP
PIECE = D // NTP
EXTRA = 16
UNITS = 704
norm_eps = 1e-06
gate_power = 8.0
bf16, f32 = jnp.bfloat16, jnp.float32


def moved(value, axis, n, by):
    return lax.ppermute(value, axis, [(i, (i + by) % n) for i in range(n)])


def ring_gathered(block, axis, n):
    got = [block] + [None] * (n - 1)
    ahead = back = block
    for s in range(1, n // 2):
        ahead = moved(ahead, axis, n, 1)
        back = moved(back, axis, n, -1)
        got[s], got[n - s] = ahead, back
    half = block.shape[0] // 2
    first = moved(ahead[:half], axis, n, 1)
    second = moved(back[half:], axis, n, -1)
    got[n // 2] = jnp.concatenate([first, second], axis=0)
    return got


def swapped(value):
    return lax.ppermute(value, "c", [(0, 1), (1, 0)])


def spread(value, axis, n):
    pairs = [(2 * i, 2 * ((i + 1) % n)) for i in range(n)]
    pairs += [(2 * i + 1, 2 * ((i - 1) % n) + 1) for i in range(n)]
    return lax.ppermute(value, (axis, "c"), pairs)


def ring_pieces(pack, axis, n):
    p = [pack]
    for _ in range(1, n // 2):
        p.append(spread(p[-1], axis, n))
    return p, spread(p[-1][0], axis, n)


def rows_ring(pack):
    p, far = ring_pieces(pack, "y", NY)
    return [p[0], p[1], far, swapped(p[1]), swapped(far)]


Y_ORDER = (
    (0, 0, 0, 0), (0, 1, 0, 1), (1, 0, 1, 0), (1, 1, 1, 1),
    (2, None, 2, 0), (4, None, 2, 1), (3, 1, 3, 0), (3, 0, 3, 1),
)


def reduced_rows(give_far, give_next, keep_far, keep_next, home):
    far = (keep_far.astype(f32) + swapped(give_far).astype(f32)).astype(bf16)
    far = spread(far, "y", NY)
    follow = keep_next.astype(f32) + swapped(give_next).astype(f32)
    follow = jnp.concatenate([follow[:OWN] + far.astype(f32), follow[OWN:]], axis=0).astype(bf16)
    return (home.astype(f32) + spread(follow, "y", NY).astype(f32)).astype(bf16)


def gelu(v):
    return 0.5 * v * (1.0 + jnp.tanh(0.7978845608028654 * (v + 0.044715 * v * v * v)))


def one_less_exp(u):
    s = 1.0 + u * (1.0 / 8.0)
    for k in range(7, 1, -1):
        s = 1.0 + u * (1.0 / k) * s
    return jnp.where(u > -0.5, -u * s, 1.0 - jnp.exp(u))


def shifted_down(values, by, rows):
    return jnp.where(rows >= by, pltpu.roll(values, by, 0), 0.0)


def stretch(index, size):
    return pl.ds(pl.multiple_of(index * size, size), size)


def upstream(axis, n, k):
    sign = 1 - 2 * lax.axis_index("c")
    return lax.rem(lax.axis_index(axis) + n - k * sign, n)


def core(rel):
    return lax.axis_index("c") if rel == 0 else 1 - lax.axis_index("c")


def dot_nt(a, b):
    return lax.dot_general(a, b, (((1,), (1,)), ((), ())), preferred_element_type=f32)


def projected(hid_ref, turned_ref, wout_ref, outs):
    my = lax.axis_index("y")
    sign = 1 - 2 * lax.axis_index("c")
    ahead, behind = lax.rem(my + NY + sign, NY), lax.rem(my + NY - sign, NY)
    across = lax.rem(my + 2, NY)
    order = [
        (across, 1), (behind, 1), (behind, 0), (across, 0), (ahead, 0), (ahead, 1), (my, 0), (my, 1),
    ]
    for i, (chip, rel) in enumerate(order):
        turned_ref[i * OWN : (i + 1) * OWN, :] = hid_ref[stretch(chip * NC + core(rel), OWN), :]

    def columns(k, _):
        at = stretch(k, PIECE)
        part = dot_nt(turned_ref[...], wout_ref[at, :]).astype(bf16)
        first = 0
        for ref in outs:
            ref[:, at] = part[first : first + ref.shape[0], :]
            first += ref.shape[0]
        return 0

    lax.fori_loop(0, NTP, columns, 0)


def behind(me, by, n):
    return lax.rem(me + (n - by), n)


def mixer_kernel(*refs):
    x_refs, w_refs = refs[0:5], refs[5:9]
    taps_ref, recur_ref, inject_ref, slope_ref = refs[9:13]
    outs, own_ref, gain_ref = refs[13:18], refs[18], refs[19]
    win_ref, wout_ref, keep_ref, drive_ref, hid_ref, turned_ref = refs[20:]
    mz, mx = lax.axis_index("z"), lax.axis_index("x")

    def placed(kz, _):
        for kx in range(NX):
            z, x = lax.rem(mz + NZ - kz, NZ), behind(mx, kx, NX)
            win_ref[z, x] = w_refs[kx][kz, :, 0:512]
            wout_ref[pl.ds(pl.multiple_of((z * NX + x) * 64, 64), 64), :] = w_refs[kx][kz, :, 512:]
        return 0

    lax.fori_loop(0, NZ, placed, 0)
    xs = []
    for operand, entry, ky, rel in Y_ORDER:
        ref = x_refs[operand] if entry is None else x_refs[operand].at[entry]
        xs.append((ref, upstream("y", NY, ky) * NC + core(rel)))
    squares = jnp.zeros((ROWS, 1), f32)
    for ref, column in xs:
        v = ref[0:ROWS, :].astype(f32)
        squares = squares + jnp.sum(v * v, axis=1, keepdims=True)
        at = stretch(column, PIECE)
        for rel in (0, 1):
            own_ref[rel * OWN : (rel + 1) * OWN, at] = ref[
                stretch(lax.axis_index("y") * NC + core(rel), OWN), :
            ]
        gain_ref[:, at] = ref[ROWS : ROWS + 8, :]
    factor = lax.rsqrt(squares / D + norm_eps)
    both = jnp.zeros((ROWS, 2 * PIECE), f32)
    for ref, column in xs:
        gain = ref[ROWS : ROWS + 1, :].astype(f32)
        v = (ref[0:ROWS, :].astype(f32) * factor * gain).astype(bf16)
        both = both + jnp.dot(v, win_ref[column].reshape(PIECE, 512), preferred_element_type=f32)
    gate_rows = both[:, 0:PIECE].astype(bf16)
    input_rows = both[:, PIECE:].astype(bf16).astype(f32)
    rows = lax.broadcasted_iota(jnp.int32, (ROWS, PIECE), 0)
    taps = taps_ref[...].astype(f32)
    smoothed = input_rows * taps[3:4, :]
    for back in (1, 2, 3):
        smoothed = smoothed + shifted_down(input_rows, back, rows) * taps[3 - back : 4 - back, :]
    smoothed = smoothed.astype(bf16)
    recur = jax.nn.sigmoid(jnp.dot(smoothed, recur_ref[...], preferred_element_type=f32))
    inject = jax.nn.sigmoid(jnp.dot(smoothed, inject_ref[...], preferred_element_type=f32))
    log_retain = -gate_power * recur * slope_ref[...]
    keep = jnp.exp(log_retain)
    drive = jnp.sqrt(one_less_exp(2.0 * log_retain)) * inject * smoothed.astype(f32)
    within = rows % 8
    for by in (1, 2, 4):
        ok = within >= by
        drive = jnp.where(ok, keep * pltpu.roll(drive, by, 0), 0.0) + drive
        keep = jnp.where(ok, pltpu.roll(keep, by, 0), 1.0) * keep
    keep_ref[...] = keep
    drive_ref[...] = drive

    def tile(i, carry):
        at = pl.ds(pl.multiple_of(i * 8, 8), 8)
        state = keep_ref[at, :] * carry + drive_ref[at, :]
        drive_ref[at, :] = state
        return state[7:8, :]

    lax.fori_loop(0, ROWS // 8, tile, jnp.zeros((1, PIECE), f32), unroll=8)
    hid_ref[...] = (gelu(gate_rows.astype(f32)) * drive_ref[...]).astype(bf16)
    projected(hid_ref, turned_ref, wout_ref, outs)


VMEM = pl.BlockSpec(memory_space=pltpu.VMEM)
PARTS = tuple(jax.ShapeDtypeStruct((n * OWN, D), bf16) for n in (1, 2, 1, 2, 2))
PAIR = jax.ShapeDtypeStruct((2 * OWN, D), bf16)


def mixer(operands):
    return pl.pallas_call(
        mixer_kernel,
        out_shape=(*PARTS, PAIR, jax.ShapeDtypeStruct((8, D), bf16)),
        in_specs=[VMEM] * len(operands),
        out_specs=(VMEM,) * 7,
        scratch_shapes=[
            pltpu.VMEM((NZ, NX, 64, 512), bf16),
            pltpu.VMEM((D, PIECE), bf16),
            pltpu.VMEM((ROWS, PIECE), f32),
            pltpu.VMEM((ROWS, PIECE), f32),
            pltpu.VMEM((ROWS, PIECE), bf16),
            pltpu.VMEM((ROWS, PIECE), bf16),
        ],
        compiler_params=pltpu.CompilerParams(vmem_limit_bytes=24 * 1024 * 1024),
        cost_estimate=pl.CostEstimate(
            flops=2 * ROWS * D * 768 + 4 * ROWS * PIECE * PIECE,
            bytes_accessed=8 * 1024 * 1024, transcendentals=ROWS * PIECE * 6,
        ),
        name="mixer",
    )(*operands)


def row_normed(widened, row_gain):
    factor = lax.rsqrt(jnp.sum(widened * widened, axis=1, keepdims=True) / D + norm_eps)
    return widened * factor * row_gain.astype(f32)


def between_kernel(part_ref, turned_ref, own_ref, gain_ref, middle_ref, normed_ref, hold_ref):
    total = part_ref[...].astype(f32) + turned_ref[...].astype(f32)
    middle = own_ref[...].astype(f32) + row_normed(total, gain_ref[1:2, :])
    middle = middle.astype(bf16)
    middle_ref[...] = middle
    hold_ref[...] = row_normed(middle.astype(f32), gain_ref[2:3, :]).astype(bf16).astype(f32)
    mz, mx = lax.axis_index("z"), lax.axis_index("x")
    for j in range(NZ):
        v = hold_ref[:, stretch(lax.rem(mz + j, NZ), 256)]
        v = pltpu.roll(v, lax.rem(256 - 64 * mx, 256), 1).astype(bf16)
        for rel in (0, 1):
            normed_ref[rel, :, j * 256 : (j + 1) * 256] = v[rel * OWN : (rel + 1) * OWN, :]


def between(part, turned, own_rows, gain_rows):
    return pl.pallas_call(
        between_kernel,
        out_shape=(PAIR, jax.ShapeDtypeStruct((2, OWN, D), bf16)),
        in_specs=[VMEM] * 4,
        out_specs=(VMEM, VMEM),
        scratch_shapes=[pltpu.VMEM((2 * OWN, D), f32)],
        cost_estimate=pl.CostEstimate(
            flops=2 * OWN * D * 20, bytes_accessed=3 * 1024 * 1024, transcendentals=256
        ),
        name="between",
    )(part, turned, own_rows, gain_rows)


UP_CUT = 256
UP_CUTS = 6
TOP = 16


def ffn_kernel(*refs):
    n_refs, u_refs, d_refs, taps_ref = refs[0:5], refs[5:13], refs[13:17], refs[17]
    outs = refs[18:23]
    n_all, down_w, up_ref, act_ref, turned_ref, sems = refs[23:]
    mz, mx = lax.axis_index("z"), lax.axis_index("x")
    downs = []
    for kz in range(NZ):
        for kx in range(NX):
            at = stretch(behind(mz, kz, NZ) * NX + behind(mx, kx, NX), 64)
            downs.append(
                pltpu.make_async_copy(d_refs[kx].at[kz], down_w.at[at, :], sems.at[len(downs)])
            )
    for copy in downs:
        copy.start()
    for operand, entry, ky, rel in Y_ORDER:
        ref = n_refs[operand] if entry is None else n_refs[operand].at[entry]
        n_all[stretch(upstream("y", NY, ky) * NC + core(rel), OWN), :] = ref[...]
    up_ref[0:TOP, :] = jnp.zeros((TOP, 2 * UNITS), bf16)

    def up(at, size):
        total = jnp.zeros((ROWS, size), f32)
        for j in range(NZ):
            w = u_refs[j][:, :, at].reshape(256, size)
            total = total + jnp.dot(
                n_all[:, j * 256 : (j + 1) * 256], w, preferred_element_type=f32
            )
        up_ref[TOP:, at] = total.astype(bf16)

    def loop(i, _):
        up(stretch(i, UP_CUT), UP_CUT)
        return 0

    lax.fori_loop(0, UP_CUTS - 1, loop, 0)
    up(pl.ds((UP_CUTS - 1) * UP_CUT, 128), 128)
    taps = taps_ref[...].astype(f32)

    def smooth(i, _):
        at = pl.multiple_of(i * 64, 64)
        v = up_ref[pl.ds(at, 64 + TOP), :].astype(f32)
        conv = v[TOP:] * taps[2:3, :]
        for back in (1, 2):
            conv = conv + pltpu.roll(v, back, 0)[TOP:] * taps[2 - back : 3 - back, :]
        act_ref[pl.ds(at, 64), :] = (gelu(conv[:, 0:UNITS]) * conv[:, UNITS:]).astype(bf16)
        return 0

    lax.fori_loop(0, ROWS // 64, smooth, 0)
    for copy in downs:
        copy.wait()
    projected(act_ref, turned_ref, down_w, outs)


def ffn(operands):
    return pl.pallas_call(
        ffn_kernel,
        out_shape=PARTS,
        in_specs=[VMEM] * 13 + [pl.BlockSpec(memory_space=pl.ANY)] * 4 + [VMEM],
        out_specs=(VMEM,) * 5,
        scratch_shapes=[
            pltpu.VMEM((ROWS, D), bf16),
            pltpu.VMEM((D, UNITS), bf16),
            pltpu.VMEM((ROWS + TOP, 2 * UNITS), bf16),
            pltpu.VMEM((ROWS, UNITS), bf16),
            pltpu.VMEM((ROWS, UNITS), bf16),
            pltpu.SemaphoreType.DMA((NZ * NX,)),
        ],
        compiler_params=pltpu.CompilerParams(vmem_limit_bytes=36 * 1024 * 1024),
        cost_estimate=pl.CostEstimate(
            flops=2 * ROWS * D * 3 * UNITS, bytes_accessed=13 * 1024 * 1024,
            transcendentals=ROWS * UNITS,
        ),
        name="ffn",
    )(*operands)


def ahead_order(blocks):
    return [blocks[-k] for k in range(len(blocks))]


def shards(
    tokens, pre_mix_gain, w_gate_in, w_input, mix_kernel, w_recur, w_inject, decay_param,
    w_mix_out, post_mix_gain, pre_ffn_gain, w_up_gate, w_up_value, gate_kernel, value_kernel,
    w_down, post_ffn_gain,
):
    gains = jnp.stack([pre_mix_gain, post_mix_gain, pre_ffn_gain, post_ffn_gain])
    packed = jnp.concatenate([tokens, jnp.pad(gains, ((0, EXTRA - 4), (0, 0)))], axis=0)
    z_own = jnp.concatenate([w_gate_in, w_input, w_mix_out.T, w_down.T], axis=1)
    along_z = ring_gathered(z_own, "z", NZ)
    mix_blocks = ring_gathered(jnp.stack([b[:, :768] for b in along_z]), "x", NX)
    x_blocks = rows_ring(jnp.stack([packed, swapped(packed)]))
    up_own = jnp.concatenate([w_up_gate, w_up_value], axis=1)
    along_x = jnp.stack(ahead_order(ring_gathered(up_own, "x", NX)))
    up_blocks = ahead_order(ring_gathered(along_x, "z", NZ))
    down_blocks = ring_gathered(jnp.stack([b[:, 768:] for b in along_z]), "x", NX)
    slope = jax.nn.softplus(-decay_param)[None, :]
    *parts, own_rows, gain_rows = mixer(
        (*x_blocks, *mix_blocks, mix_kernel, w_recur[0], w_inject[0], slope)
    )
    part = reduced_rows(*parts)
    turned = swapped(jnp.concatenate([part[OWN:], part[:OWN]], axis=0))
    middle, normed = between(part, turned, own_rows, gain_rows)
    taps = jnp.concatenate([gate_kernel, value_kernel], axis=1)
    parts = ffn((*rows_ring(normed), *up_blocks, *down_blocks, taps))
    part = reduced_rows(*parts)
    ffn_sum = part[:OWN].astype(f32) + swapped(part[OWN:]).astype(f32)
    out_rows = middle[:OWN].astype(f32) + row_normed(ffn_sum, gain_rows[3:4])
    to_columns = out_rows.astype(bf16).reshape(OWN, NTP, PIECE).transpose(1, 0, 2)
    return lax.all_to_all(to_columns, TP, 0, 0, tiled=True).reshape(ROWS, PIECE)


def solution(mesh):
    finer = Mesh(mesh.devices.reshape(NZ, NX, NY, NC), ("z", "x", "y", "c"))
    return jax.shard_map(
        shards,
        mesh=finer,
        in_specs=(
            P(FS, TP), P(TP), P(FS, TP), P(FS, TP), P(None, TP), P(TP, None, None),
            P(TP, None, None), P(TP), P(TP, FS), P(TP), P(TP), P(FS, TP), P(FS, TP),
            P(None, TP), P(None, TP), P(TP, FS), P(TP),
        ),
        out_specs=P(FS, TP),
        check_vma=False,
    )
```

```python
import jax
import jax.numpy as jnp
from jax import lax
from jax.experimental import pallas as pl
from jax.experimental.pallas import tpu as pltpu
from jax.sharding import Mesh
from jax.sharding import PartitionSpec as P


D = 2048
FS = ("z", "x")
TP = ("y", "c")
NZ, NX, NY, NC = 8, 4, 4, 2
NTP = NY * NC
ROWS = 512
OWN = ROWS // NTP
PIECE = D // NTP
EXTRA = 16
UNITS = 704
norm_eps = 1e-06
gate_power = 8.0
bf16, f32 = jnp.bfloat16, jnp.float32


def moved(value, axis, n, by):
    return lax.ppermute(value, axis, [(i, (i + by) % n) for i in range(n)])


def ring_gathered(block, axis, n):
    got = [block] + [None] * (n - 1)
    ahead = back = block
    for s in range(1, n // 2):
        ahead = moved(ahead, axis, n, 1)
        back = moved(back, axis, n, -1)
        got[s], got[n - s] = ahead, back
    far = jnp.where(lax.axis_index("c") == 0, ahead, back)
    got[n // 2] = spread(far, axis, n)
    return got


def in_order(blocks, axis, dim):
    n, me = len(blocks), lax.axis_index(axis)
    shape = blocks[0].shape
    whole = jnp.zeros((*shape[:dim], n, *shape[dim:]), blocks[0].dtype)
    for k, block in enumerate(blocks):
        start = [0] * whole.ndim
        start[dim] = lax.rem(me + (n - k), n)
        whole = lax.dynamic_update_slice(whole, jnp.expand_dims(block, dim), start)
    return whole


def swapped(value):
    return lax.ppermute(value, "c", [(0, 1), (1, 0)])


def spread(value, axis, n):
    pairs = [(2 * i, 2 * ((i + 1) % n)) for i in range(n)]
    pairs += [(2 * i + 1, 2 * ((i - 1) % n) + 1) for i in range(n)]
    return lax.ppermute(value, (axis, "c"), pairs)


def ring_pieces(pack, axis, n):
    p = [pack]
    for _ in range(1, n // 2):
        p.append(spread(p[-1], axis, n))
    return p, spread(p[-1][0], axis, n)


def rows_ring(pack):
    p, far = ring_pieces(pack, "y", NY)
    return [p[0], p[1], far, swapped(p[1]), swapped(far)]


Y_ORDER = (
    (0, 0, 0, 0), (0, 1, 0, 1), (1, 0, 1, 0), (1, 1, 1, 1),
    (2, None, 2, 0), (4, None, 2, 1), (3, 1, 3, 0), (3, 0, 3, 1),
)


def reduced_rows(give, keep_far, keep_next, home):
    given = swapped(give).astype(f32)
    far = (keep_far.astype(f32) + given[:OWN]).astype(bf16)
    far = spread(far, "y", NY)
    follow = keep_next.astype(f32) + given[OWN:]
    follow = jnp.concatenate([follow[:OWN] + far.astype(f32), follow[OWN:]], axis=0).astype(bf16)
    return (home.astype(f32) + spread(follow, "y", NY).astype(f32)).astype(bf16)


def gelu(v):
    return 0.5 * v * (1.0 + jnp.tanh(0.7978845608028654 * (v + 0.044715 * v * v * v)))


def one_less_exp(u):
    s = 1.0 + u * (1.0 / 8.0)
    for k in range(7, 1, -1):
        s = 1.0 + u * (1.0 / k) * s
    return jnp.where(u > -0.5, -u * s, 1.0 - jnp.exp(u))


def stretch(index, size):
    return pl.ds(pl.multiple_of(index * size, size), size)


def upstream(axis, n, k):
    sign = 1 - 2 * lax.axis_index("c")
    return lax.rem(lax.axis_index(axis) + n - k * sign, n)


def core(rel):
    return lax.axis_index("c") if rel == 0 else 1 - lax.axis_index("c")


def dot_nt(a, b):
    return lax.dot_general(a, b, (((1,), (1,)), ((), ())), preferred_element_type=f32)


def projected(hid_ref, turned_ref, wout_ref, outs):
    my = lax.axis_index("y")
    sign = 1 - 2 * lax.axis_index("c")
    ahead, behind = lax.rem(my + NY + sign, NY), lax.rem(my + NY - sign, NY)
    across = lax.rem(my + 2, NY)
    order = [
        (across, 1), (behind, 1), (behind, 0), (across, 0), (ahead, 0), (ahead, 1), (my, 0), (my, 1),
    ]
    for i, (chip, rel) in enumerate(order):
        turned_ref[i * OWN : (i + 1) * OWN, :] = hid_ref[stretch(chip * NC + core(rel), OWN), :]

    def columns(k, _):
        at = stretch(k, PIECE)
        part = dot_nt(turned_ref[...], wout_ref[at, :]).astype(bf16)
        first = 0
        for ref in outs:
            ref[:, at] = part[first : first + ref.shape[0], :]
            first += ref.shape[0]
        return 0

    lax.fori_loop(0, NTP, columns, 0)


def behind(me, by, n):
    return lax.rem(me + (n - by), n)


def mixer_kernel(*refs):
    x_refs, w_refs = refs[0:5], refs[5:9]
    taps_ref, recur_ref, inject_ref, slope_ref = refs[9:13]
    outs, own_ref, gain_ref = refs[13:17], refs[17], refs[18]
    v_ref, win_ref, wout_ref, gate_ref, in_ref, keep_ref, drive_ref, hid_ref, turned_ref = refs[19:]
    mz, mx = lax.axis_index("z"), lax.axis_index("x")

    def placed(kz, _):
        for kx in range(NX):
            z, x = lax.rem(mz + NZ - kz, NZ), behind(mx, kx, NX)
            at = pl.ds(pl.multiple_of((z * NX + x) * 64, 64), 64)
            win_ref[at, :] = w_refs[kx][kz, :, 0:512]
            wout_ref[at, :] = w_refs[kx][kz, :, 512:]
        return 0

    lax.fori_loop(0, NZ, placed, 0)
    xs = []
    for operand, entry, ky, rel in Y_ORDER:
        ref = x_refs[operand] if entry is None else x_refs[operand].at[entry]
        xs.append((ref, stretch(upstream("y", NY, ky) * NC + core(rel), PIECE)))
    for ref, at in xs:
        for rel in (0, 1):
            own_ref[rel * OWN : (rel + 1) * OWN, at] = ref[
                stretch(lax.axis_index("y") * NC + core(rel), OWN), :
            ]
        gain_ref[:, at] = ref[ROWS : ROWS + 8, :]

    def normed(i, _):
        rows = stretch(i, 64)
        squares = jnp.zeros((64, 1), f32)
        for ref, _at in xs:
            v = ref[rows, :].astype(f32)
            squares = squares + jnp.sum(v * v, axis=1, keepdims=True)
        factor = lax.rsqrt(squares / D + norm_eps)
        for ref, at in xs:
            gain = ref[ROWS : ROWS + 1, :].astype(f32)
            v_ref[rows, at] = (ref[rows, :].astype(f32) * factor * gain).astype(bf16)
        return 0

    lax.fori_loop(0, ROWS // 64, normed, 0)
    gate_ref[...] = jnp.dot(
        v_ref[...], win_ref[:, 0:PIECE], preferred_element_type=f32
    ).astype(bf16)
    in_ref[0:TOP, :] = jnp.zeros((TOP, PIECE), bf16)
    in_ref[TOP:, :] = jnp.dot(
        v_ref[...], win_ref[:, PIECE:], preferred_element_type=f32
    ).astype(bf16)
    taps = taps_ref[...].astype(f32)
    within = lax.broadcasted_iota(jnp.int32, (CHUNK, PIECE), 0) % 8

    def chunk(i, carry):
        first = pl.multiple_of(i * CHUNK, CHUNK)
        rows = pl.ds(first, CHUNK)
        v = in_ref[pl.ds(first, CHUNK + TOP), :].astype(f32)
        smoothed = v[TOP:] * taps[3:4, :]
        for back in (1, 2, 3):
            smoothed = smoothed + pltpu.roll(v, back, 0)[TOP:] * taps[3 - back : 4 - back, :]
        smoothed = smoothed.astype(bf16)
        recur = jax.nn.sigmoid(jnp.dot(smoothed, recur_ref[...], preferred_element_type=f32))
        inject = jax.nn.sigmoid(jnp.dot(smoothed, inject_ref[...], preferred_element_type=f32))
        log_retain = -gate_power * recur * slope_ref[...]
        keep = jnp.exp(log_retain)
        drive = jnp.sqrt(one_less_exp(2.0 * log_retain)) * inject * smoothed.astype(f32)
        for by in (1, 2, 4):
            ok = within >= by
            drive = jnp.where(ok, keep * pltpu.roll(drive, by, 0), 0.0) + drive
            keep = jnp.where(ok, pltpu.roll(keep, by, 0), 1.0) * keep
        keep_ref[...] = keep
        drive_ref[...] = drive
        for t in range(CHUNK // 8):
            at = slice(8 * t, 8 * t + 8)
            state = keep_ref[at, :] * carry + drive_ref[at, :]
            drive_ref[at, :] = state
            carry = state[7:8, :]
        hid_ref[rows, :] = (gelu(gate_ref[rows, :].astype(f32)) * drive_ref[...]).astype(bf16)
        return carry

    lax.fori_loop(0, ROWS // CHUNK, chunk, jnp.zeros((1, PIECE), f32))
    projected(hid_ref, turned_ref, wout_ref, outs)


CHUNK = 128
TOP = 16
VMEM = pl.BlockSpec(memory_space=pltpu.VMEM)
PARTS = tuple(jax.ShapeDtypeStruct((n * OWN, D), bf16) for n in (3, 1, 2, 2))
PAIR = jax.ShapeDtypeStruct((2 * OWN, D), bf16)


def mixer(operands):
    return pl.pallas_call(
        mixer_kernel,
        out_shape=(*PARTS, PAIR, jax.ShapeDtypeStruct((8, D), bf16)),
        in_specs=[VMEM] * len(operands),
        out_specs=(VMEM,) * 6,
        scratch_shapes=[
            pltpu.VMEM((ROWS, D), bf16),
            pltpu.VMEM((D, 512), bf16),
            pltpu.VMEM((D, PIECE), bf16),
            pltpu.VMEM((ROWS, PIECE), bf16),
            pltpu.VMEM((ROWS + TOP, PIECE), bf16),
            pltpu.VMEM((CHUNK, PIECE), f32),
            pltpu.VMEM((CHUNK, PIECE), f32),
            pltpu.VMEM((ROWS, PIECE), bf16),
            pltpu.VMEM((ROWS, PIECE), bf16),
        ],
        compiler_params=pltpu.CompilerParams(vmem_limit_bytes=24 * 1024 * 1024),
        cost_estimate=pl.CostEstimate(
            flops=2 * ROWS * D * 768 + 4 * ROWS * PIECE * PIECE,
            bytes_accessed=8 * 1024 * 1024, transcendentals=ROWS * PIECE * 6,
        ),
        name="mixer",
    )(*operands)


def row_normed(widened, row_gain):
    factor = lax.rsqrt(jnp.sum(widened * widened, axis=1, keepdims=True) / D + norm_eps)
    return widened * factor * row_gain.astype(f32)


UP_CUT = 256
UP_CUTS = 6


def ffn_kernel(*refs):
    n_refs, up_w, down_w, taps_ref = refs[0:5], refs[5], refs[6], refs[7]
    outs = refs[8:12]
    n_all, up_ref, act_ref, turned_ref = refs[12:]
    for operand, entry, ky, rel in Y_ORDER:
        ref = n_refs[operand] if entry is None else n_refs[operand].at[entry]
        n_all[stretch(upstream("y", NY, ky) * NC + core(rel), OWN), :] = ref[...]
    up_ref[0:TOP, :] = jnp.zeros((TOP, 2 * UNITS), bf16)

    def up(at):
        up_ref[TOP:, at] = jnp.dot(
            n_all[...], up_w[:, at], preferred_element_type=f32
        ).astype(bf16)

    def loop(i, _):
        up(stretch(i, UP_CUT))
        return 0

    lax.fori_loop(0, UP_CUTS - 1, loop, 0)
    up(pl.ds((UP_CUTS - 1) * UP_CUT, 128))
    taps = taps_ref[...].astype(f32)

    def smooth(i, _):
        at = pl.multiple_of(i * 64, 64)
        v = up_ref[pl.ds(at, 64 + TOP), :].astype(f32)
        conv = v[TOP:] * taps[2:3, :]
        for back in (1, 2):
            conv = conv + pltpu.roll(v, back, 0)[TOP:] * taps[2 - back : 3 - back, :]
        act_ref[pl.ds(at, 64), :] = (gelu(conv[:, 0:UNITS]) * conv[:, UNITS:]).astype(bf16)
        return 0

    lax.fori_loop(0, ROWS // 64, smooth, 0)
    projected(act_ref, turned_ref, down_w, outs)


def ffn(operands):
    return pl.pallas_call(
        ffn_kernel,
        out_shape=PARTS,
        in_specs=[VMEM] * 8,
        out_specs=(VMEM,) * 4,
        scratch_shapes=[
            pltpu.VMEM((ROWS, D), bf16),
            pltpu.VMEM((ROWS + TOP, 2 * UNITS), bf16),
            pltpu.VMEM((ROWS, UNITS), bf16),
            pltpu.VMEM((ROWS, UNITS), bf16),
        ],
        compiler_params=pltpu.CompilerParams(vmem_limit_bytes=28 * 1024 * 1024),
        cost_estimate=pl.CostEstimate(
            flops=2 * ROWS * D * 3 * UNITS, bytes_accessed=13 * 1024 * 1024,
            transcendentals=ROWS * UNITS,
        ),
        name="ffn",
    )(*operands)


def shards(
    tokens, pre_mix_gain, w_gate_in, w_input, mix_kernel, w_recur, w_inject, decay_param,
    w_mix_out, post_mix_gain, pre_ffn_gain, w_up_gate, w_up_value, gate_kernel, value_kernel,
    w_down, post_ffn_gain,
):
    gains = jnp.stack([pre_mix_gain, post_mix_gain, pre_ffn_gain, post_ffn_gain])
    packed = jnp.concatenate([tokens, jnp.pad(gains, ((0, EXTRA - 4), (0, 0)))], axis=0)
    z_own = jnp.concatenate([w_gate_in, w_input, w_mix_out.T, w_down.T], axis=1)
    along_z = ring_gathered(z_own, "z", NZ)
    mix_blocks = ring_gathered(jnp.stack([b[:, :768] for b in along_z]), "x", NX)
    x_blocks = rows_ring(jnp.stack([packed, swapped(packed)]))
    up_own = jnp.concatenate([w_up_gate, w_up_value], axis=1)
    along_x = in_order(ring_gathered(up_own, "x", NX), "x", 0)
    up_all = in_order(ring_gathered(along_x, "z", NZ), "z", 0).reshape(D, 2 * UNITS)
    down_z = in_order([b[:, 768:] for b in along_z], "z", 0)
    down_all = in_order(ring_gathered(down_z, "x", NX), "x", 1).reshape(D, UNITS)
    slope = jax.nn.softplus(-decay_param)[None, :]
    *parts, own_rows, gain_rows = mixer(
        (*x_blocks, *mix_blocks, mix_kernel, w_recur[0], w_inject[0], slope)
    )
    part = reduced_rows(*parts)
    turned = swapped(jnp.concatenate([part[OWN:], part[:OWN]], axis=0))
    mixer_sum = part.astype(f32) + turned.astype(f32)
    middle = (own_rows.astype(f32) + row_normed(mixer_sum, gain_rows[1:2])).astype(bf16)
    normed = row_normed(middle.astype(f32), gain_rows[2:3]).astype(bf16).reshape(2, OWN, D)
    taps = jnp.concatenate([gate_kernel, value_kernel], axis=1)
    parts = ffn((*rows_ring(normed), up_all, down_all, taps))
    part = reduced_rows(*parts)
    ffn_sum = part[:OWN].astype(f32) + swapped(part[OWN:]).astype(f32)
    out_rows = middle[:OWN].astype(f32) + row_normed(ffn_sum, gain_rows[3:4])
    to_columns = out_rows.astype(bf16).reshape(OWN, NTP, PIECE).transpose(1, 0, 2)
    return lax.all_to_all(to_columns, TP, 0, 0, tiled=True).reshape(ROWS, PIECE)


def solution(mesh):
    finer = Mesh(mesh.devices.reshape(NZ, NX, NY, NC), ("z", "x", "y", "c"))
    return jax.shard_map(
        shards,
        mesh=finer,
        in_specs=(
            P(FS, TP), P(TP), P(FS, TP), P(FS, TP), P(None, TP), P(TP, None, None),
            P(TP, None, None), P(TP), P(TP, FS), P(TP), P(TP), P(FS, TP), P(FS, TP),
            P(None, TP), P(None, TP), P(TP, FS), P(TP),
        ),
        out_specs=P(FS, TP),
        check_vma=False,
    )
```

```python
import jax
import jax.numpy as jnp
from jax import lax
from jax.experimental import pallas as pl
from jax.experimental.pallas import tpu as pltpu
from jax.sharding import Mesh
from jax.sharding import PartitionSpec as P


D = 2048
FS = ("z", "x")
TP = ("y", "c")
NZ, NX, NY, NC = 8, 4, 4, 2
NTP = NY * NC
ROWS = 512
OWN = ROWS // NTP
PIECE = D // NTP
EXTRA = 16
UNITS = 704
norm_eps = 1e-06
gate_power = 8.0
bf16, f32 = jnp.bfloat16, jnp.float32


def moved(value, axis, n, by):
    return lax.ppermute(value, axis, [(i, (i + by) % n) for i in range(n)])


def ring_gathered(block, axis, n):
    got = [block] + [None] * (n - 1)
    ahead = back = block
    for s in range(1, n // 2):
        ahead = moved(ahead, axis, n, 1)
        back = moved(back, axis, n, -1)
        got[s], got[n - s] = ahead, back
    far = jnp.where(lax.axis_index("c") == 0, ahead, back)
    got[n // 2] = spread(far, axis, n)
    return got


def in_order(blocks, axis, dim):
    n, me = len(blocks), lax.axis_index(axis)
    shape = blocks[0].shape
    whole = jnp.zeros((*shape[:dim], n, *shape[dim:]), blocks[0].dtype)
    for k in [1, 0, *range(2, n)]:
        start = [0] * whole.ndim
        start[dim] = lax.rem(me + (n - k), n)
        whole = lax.dynamic_update_slice(whole, jnp.expand_dims(blocks[k], dim), start)
    return whole


def swapped(value):
    return lax.ppermute(value, "c", [(0, 1), (1, 0)])


def spread(value, axis, n):
    pairs = [(2 * i, 2 * ((i + 1) % n)) for i in range(n)]
    pairs += [(2 * i + 1, 2 * ((i - 1) % n) + 1) for i in range(n)]
    return lax.ppermute(value, (axis, "c"), pairs)


def ring_pieces(pack, axis, n):
    p = [pack]
    for _ in range(1, n // 2):
        p.append(spread(p[-1], axis, n))
    return p, spread(p[-1][0], axis, n)


def rows_ring(pack):
    p, far = ring_pieces(pack, "y", NY)
    return [p[0], p[1], far, swapped(p[1]), swapped(far)]


Y_ORDER = (
    (0, 0, 0, 0), (0, 1, 0, 1), (1, 0, 1, 0), (1, 1, 1, 1),
    (2, None, 2, 0), (4, None, 2, 1), (3, 1, 3, 0), (3, 0, 3, 1),
)


def reduced_rows(give, keep_far, keep_next, home):
    given = swapped(give).astype(f32)
    far = (keep_far.astype(f32) + given[:OWN]).astype(bf16)
    far = spread(far, "y", NY)
    follow = keep_next.astype(f32) + given[OWN:]
    follow = jnp.concatenate([follow[:OWN] + far.astype(f32), follow[OWN:]], axis=0).astype(bf16)
    return (home.astype(f32) + spread(follow, "y", NY).astype(f32)).astype(bf16)


def gelu(v):
    return 0.5 * v * (1.0 + jnp.tanh(0.7978845608028654 * (v + 0.044715 * v * v * v)))


def one_less_exp(u):
    s = 1.0 + u * (1.0 / 8.0)
    for k in range(7, 1, -1):
        s = 1.0 + u * (1.0 / k) * s
    return jnp.where(u > -0.5, -u * s, 1.0 - jnp.exp(u))


def stretch(index, size):
    return pl.ds(pl.multiple_of(index * size, size), size)


def upstream(axis, n, k):
    sign = 1 - 2 * lax.axis_index("c")
    return lax.rem(lax.axis_index(axis) + n - k * sign, n)


def core(rel):
    return lax.axis_index("c") if rel == 0 else 1 - lax.axis_index("c")


def dot_nt(a, b):
    return lax.dot_general(a, b, (((1,), (1,)), ((), ())), preferred_element_type=f32)


def projected(hid_ref, turned_ref, wout_ref, outs):
    my = lax.axis_index("y")
    sign = 1 - 2 * lax.axis_index("c")
    ahead, behind = lax.rem(my + NY + sign, NY), lax.rem(my + NY - sign, NY)
    across = lax.rem(my + 2, NY)
    order = [
        (across, 1), (behind, 1), (behind, 0), (across, 0), (ahead, 0), (ahead, 1), (my, 0), (my, 1),
    ]
    for i, (chip, rel) in enumerate(order):
        turned_ref[i * OWN : (i + 1) * OWN, :] = hid_ref[stretch(chip * NC + core(rel), OWN), :]

    def columns(k, _):
        at = stretch(k, PIECE)
        part = dot_nt(turned_ref[...], wout_ref[at, :]).astype(bf16)
        first = 0
        for ref in outs:
            ref[:, at] = part[first : first + ref.shape[0], :]
            first += ref.shape[0]
        return 0

    lax.fori_loop(0, NTP, columns, 0)


def behind(me, by, n):
    return lax.rem(me + (n - by), n)


def mixer_kernel(*refs):
    x_refs, w_refs = refs[0:5], refs[5:9]
    taps_ref, recur_ref, inject_ref, slope_ref = refs[9:13]
    outs, own_ref, gain_ref = refs[13:17], refs[17], refs[18]
    v_ref, win_ref, wout_ref, gate_ref, in_ref, keep_ref, drive_ref, hid_ref, turned_ref = refs[19:]
    mz, mx = lax.axis_index("z"), lax.axis_index("x")

    def placed(kz, _):
        for kx in range(NX):
            z, x = lax.rem(mz + NZ - kz, NZ), behind(mx, kx, NX)
            at = pl.ds(pl.multiple_of((z * NX + x) * 64, 64), 64)
            win_ref[at, :] = w_refs[kx][kz, :, 0:512]
            wout_ref[at, :] = w_refs[kx][kz, :, 512:]
        return 0

    lax.fori_loop(0, NZ, placed, 0)
    xs = []
    for operand, entry, ky, rel in Y_ORDER:
        ref = x_refs[operand] if entry is None else x_refs[operand].at[entry]
        xs.append((ref, stretch(upstream("y", NY, ky) * NC + core(rel), PIECE)))
    for ref, at in xs:
        for rel in (0, 1):
            own_ref[rel * OWN : (rel + 1) * OWN, at] = ref[
                stretch(lax.axis_index("y") * NC + core(rel), OWN), :
            ]
        gain_ref[:, at] = ref[ROWS : ROWS + 8, :]

    def normed(i, _):
        rows = stretch(i, 64)
        squares = jnp.zeros((64, 1), f32)
        for ref, _at in xs:
            v = ref[rows, :].astype(f32)
            squares = squares + jnp.sum(v * v, axis=1, keepdims=True)
        factor = lax.rsqrt(squares / D + norm_eps)
        for ref, at in xs:
            gain = ref[ROWS : ROWS + 1, :].astype(f32)
            v_ref[rows, at] = (ref[rows, :].astype(f32) * factor * gain).astype(bf16)
        return 0

    lax.fori_loop(0, ROWS // 64, normed, 0)
    gate_ref[...] = jnp.dot(
        v_ref[...], win_ref[:, 0:PIECE], preferred_element_type=f32
    ).astype(bf16)
    in_ref[0:TOP, :] = jnp.zeros((TOP, PIECE), bf16)
    in_ref[TOP:, :] = jnp.dot(
        v_ref[...], win_ref[:, PIECE:], preferred_element_type=f32
    ).astype(bf16)
    taps = taps_ref[...].astype(f32)
    within = lax.broadcasted_iota(jnp.int32, (CHUNK, PIECE), 0) % 8

    def chunk(i, carry):
        first = pl.multiple_of(i * CHUNK, CHUNK)
        rows = pl.ds(first, CHUNK)
        v = in_ref[pl.ds(first, CHUNK + TOP), :].astype(f32)
        smoothed = v[TOP:] * taps[3:4, :]
        for back in (1, 2, 3):
            smoothed = smoothed + pltpu.roll(v, back, 0)[TOP:] * taps[3 - back : 4 - back, :]
        smoothed = smoothed.astype(bf16)
        recur = jax.nn.sigmoid(jnp.dot(smoothed, recur_ref[...], preferred_element_type=f32))
        inject = jax.nn.sigmoid(jnp.dot(smoothed, inject_ref[...], preferred_element_type=f32))
        log_retain = -gate_power * recur * slope_ref[...]
        keep = jnp.exp(log_retain)
        drive = jnp.sqrt(one_less_exp(2.0 * log_retain)) * inject * smoothed.astype(f32)
        for by in (1, 2, 4):
            ok = within >= by
            drive = jnp.where(ok, keep * pltpu.roll(drive, by, 0), 0.0) + drive
            keep = jnp.where(ok, pltpu.roll(keep, by, 0), 1.0) * keep
        keep_ref[...] = keep
        drive_ref[...] = drive
        for t in range(CHUNK // 8):
            at = slice(8 * t, 8 * t + 8)
            state = keep_ref[at, :] * carry + drive_ref[at, :]
            drive_ref[at, :] = state
            carry = state[7:8, :]
        hid_ref[rows, :] = (gelu(gate_ref[rows, :].astype(f32)) * drive_ref[...]).astype(bf16)
        return carry

    lax.fori_loop(0, ROWS // CHUNK, chunk, jnp.zeros((1, PIECE), f32))
    projected(hid_ref, turned_ref, wout_ref, outs)


CHUNK = 128
TOP = 16
VMEM = pl.BlockSpec(memory_space=pltpu.VMEM)
PARTS = tuple(jax.ShapeDtypeStruct((n * OWN, D), bf16) for n in (3, 1, 2, 2))
PAIR = jax.ShapeDtypeStruct((2 * OWN, D), bf16)


def mixer(operands):
    return pl.pallas_call(
        mixer_kernel,
        out_shape=(*PARTS, PAIR, jax.ShapeDtypeStruct((8, D), bf16)),
        in_specs=[VMEM] * len(operands),
        out_specs=(VMEM,) * 6,
        scratch_shapes=[
            pltpu.VMEM((ROWS, D), bf16),
            pltpu.VMEM((D, 512), bf16),
            pltpu.VMEM((D, PIECE), bf16),
            pltpu.VMEM((ROWS, PIECE), bf16),
            pltpu.VMEM((ROWS + TOP, PIECE), bf16),
            pltpu.VMEM((CHUNK, PIECE), f32),
            pltpu.VMEM((CHUNK, PIECE), f32),
            pltpu.VMEM((ROWS, PIECE), bf16),
            pltpu.VMEM((ROWS, PIECE), bf16),
        ],
        compiler_params=pltpu.CompilerParams(vmem_limit_bytes=24 * 1024 * 1024),
        cost_estimate=pl.CostEstimate(
            flops=2 * ROWS * D * 768 + 4 * ROWS * PIECE * PIECE,
            bytes_accessed=8 * 1024 * 1024, transcendentals=ROWS * PIECE * 6,
        ),
        name="mixer",
    )(*operands)


def row_normed(widened, row_gain):
    factor = lax.rsqrt(jnp.sum(widened * widened, axis=1, keepdims=True) / D + norm_eps)
    return widened * factor * row_gain.astype(f32)


UP_CUT = 256
UP_CUTS = 6


def ffn_kernel(*refs):
    n_refs, up_w, down_w, taps_ref = refs[0:5], refs[5], refs[6], refs[7]
    outs = refs[8:12]
    n_all, up_ref, act_ref, turned_ref = refs[12:]
    for operand, entry, ky, rel in Y_ORDER:
        ref = n_refs[operand] if entry is None else n_refs[operand].at[entry]
        n_all[stretch(upstream("y", NY, ky) * NC + core(rel), OWN), :] = ref[...]
    up_ref[0:TOP, :] = jnp.zeros((TOP, 2 * UNITS), bf16)

    def up(at):
        up_ref[TOP:, at] = jnp.dot(
            n_all[...], up_w[:, at], preferred_element_type=f32
        ).astype(bf16)

    def loop(i, _):
        up(stretch(i, UP_CUT))
        return 0

    lax.fori_loop(0, UP_CUTS - 1, loop, 0)
    up(pl.ds((UP_CUTS - 1) * UP_CUT, 128))
    taps = taps_ref[...].astype(f32)

    def smooth(i, _):
        at = pl.multiple_of(i * 64, 64)
        v = up_ref[pl.ds(at, 64 + TOP), :].astype(f32)
        conv = v[TOP:] * taps[2:3, :]
        for back in (1, 2):
            conv = conv + pltpu.roll(v, back, 0)[TOP:] * taps[2 - back : 3 - back, :]
        act_ref[pl.ds(at, 64), :] = (gelu(conv[:, 0:UNITS]) * conv[:, UNITS:]).astype(bf16)
        return 0

    lax.fori_loop(0, ROWS // 64, smooth, 0)
    projected(act_ref, turned_ref, down_w, outs)


def ffn(operands):
    return pl.pallas_call(
        ffn_kernel,
        out_shape=PARTS,
        in_specs=[VMEM] * 8,
        out_specs=(VMEM,) * 4,
        scratch_shapes=[
            pltpu.VMEM((ROWS, D), bf16),
            pltpu.VMEM((ROWS + TOP, 2 * UNITS), bf16),
            pltpu.VMEM((ROWS, UNITS), bf16),
            pltpu.VMEM((ROWS, UNITS), bf16),
        ],
        compiler_params=pltpu.CompilerParams(vmem_limit_bytes=28 * 1024 * 1024),
        cost_estimate=pl.CostEstimate(
            flops=2 * ROWS * D * 3 * UNITS, bytes_accessed=13 * 1024 * 1024,
            transcendentals=ROWS * UNITS,
        ),
        name="ffn",
    )(*operands)


def shards(
    tokens, pre_mix_gain, w_gate_in, w_input, mix_kernel, w_recur, w_inject, decay_param,
    w_mix_out, post_mix_gain, pre_ffn_gain, w_up_gate, w_up_value, gate_kernel, value_kernel,
    w_down, post_ffn_gain,
):
    z_own = jnp.concatenate([w_gate_in, w_input, w_mix_out.T, w_down.T], axis=1)
    along_z = ring_gathered(z_own, "z", NZ)
    gains = jnp.concatenate([pre_mix_gain, post_mix_gain, pre_ffn_gain, post_ffn_gain])
    gains = gains.reshape(4, PIECE)
    packed = jnp.concatenate([tokens, jnp.pad(gains, ((0, EXTRA - 4), (0, 0)))], axis=0)
    mix_blocks = ring_gathered(jnp.stack([b[:, :768] for b in along_z]), "x", NX)
    packed = jnp.stack([packed, swapped(packed)])
    x_blocks = rows_ring(packed)
    up_own = jnp.concatenate([w_up_gate, w_up_value], axis=1)
    sent = jnp.broadcast_to(up_own[None], (NX, *up_own.shape))
    along_x = lax.all_to_all(sent, "x", 0, 0, tiled=True)
    up_all = in_order(ring_gathered(along_x, "z", NZ), "z", 0).reshape(D, 2 * UNITS)
    down_z = in_order([b[:, 768:] for b in along_z], "z", 0)
    down_all = in_order(ring_gathered(down_z, "x", NX), "x", 1).reshape(D, UNITS)
    x_blocks[1], decay_param = lax.optimization_barrier((x_blocks[1], decay_param))
    slope = jax.nn.softplus(-decay_param)[None, :]
    *parts, own_rows, gain_rows = mixer(
        (*x_blocks, *mix_blocks, mix_kernel, w_recur[0], w_inject[0], slope)
    )
    part = reduced_rows(*parts)
    part, taps_of = lax.optimization_barrier((part, (gate_kernel, value_kernel)))
    taps = jnp.concatenate(taps_of, axis=1)
    turned = swapped(jnp.concatenate([part[OWN:], part[:OWN]], axis=0))
    mixer_sum = part.astype(f32) + turned.astype(f32)
    middle = (own_rows.astype(f32) + row_normed(mixer_sum, gain_rows[1:2])).astype(bf16)
    normed = row_normed(middle.astype(f32), gain_rows[2:3]).astype(bf16).reshape(2, OWN, D)
    parts = ffn((*rows_ring(normed), up_all, down_all, taps))
    part = reduced_rows(*parts)
    ffn_sum = part[:OWN].astype(f32) + swapped(part[OWN:]).astype(f32)
    out_rows = middle[:OWN].astype(f32) + row_normed(ffn_sum, gain_rows[3:4])
    to_columns = out_rows.astype(bf16).reshape(OWN, NTP, PIECE).transpose(1, 0, 2)
    return lax.all_to_all(to_columns, TP, 0, 0, tiled=True).reshape(ROWS, PIECE)


def solution(mesh):
    finer = Mesh(mesh.devices.reshape(NZ, NX, NY, NC), ("z", "x", "y", "c"))
    return jax.shard_map(
        shards,
        mesh=finer,
        in_specs=(
            P(FS, TP), P(TP), P(FS, TP), P(FS, TP), P(None, TP), P(TP, None, None),
            P(TP, None, None), P(TP), P(TP, FS), P(TP), P(TP), P(FS, TP), P(FS, TP),
            P(None, TP), P(None, TP), P(TP, FS), P(TP),
        ),
        out_specs=P(FS, TP),
        check_vma=False,
    )
```

```python
import jax
import jax.numpy as jnp
from jax import lax
from jax.experimental import pallas as pl
from jax.experimental.pallas import tpu as pltpu
from jax.sharding import Mesh
from jax.sharding import PartitionSpec as P


D = 2048
FS = ("z", "x")
TP = ("y", "c")
NZ, NX, NY, NC = 8, 4, 4, 2
NTP = NY * NC
ROWS = 512
OWN = ROWS // NTP
PIECE = D // NTP
EXTRA = 16
UNITS = 704
norm_eps = 1e-06
gate_power = 8.0
bf16, f32 = jnp.bfloat16, jnp.float32


def moved(value, axis, n, by):
    return lax.ppermute(value, axis, [(i, (i + by) % n) for i in range(n)])


def ring_gathered(block, axis, n):
    got = [block] + [None] * (n - 1)
    ahead = back = block
    for s in range(1, n // 2):
        ahead = moved(ahead, axis, n, 1)
        back = moved(back, axis, n, -1)
        got[s], got[n - s] = ahead, back
    far = jnp.where(lax.axis_index("c") == 0, ahead, back)
    got[n // 2] = spread(far, axis, n)
    return got


def in_order(blocks, axis, dim):
    n, me = len(blocks), lax.axis_index(axis)
    shape = blocks[0].shape
    whole = jnp.zeros((*shape[:dim], n, *shape[dim:]), blocks[0].dtype)
    order = [k for j in range(1, n // 2) for k in (j, n - j)] + [n // 2]
    for k in [1, 0, *order[1:]]:
        start = [0] * whole.ndim
        start[dim] = lax.rem(me + (n - k), n)
        whole = lax.dynamic_update_slice(whole, jnp.expand_dims(blocks[k], dim), start)
    return whole


def swapped(value):
    return lax.ppermute(value, "c", [(0, 1), (1, 0)])


def spread(value, axis, n):
    pairs = [(2 * i, 2 * ((i + 1) % n)) for i in range(n)]
    pairs += [(2 * i + 1, 2 * ((i - 1) % n) + 1) for i in range(n)]
    return lax.ppermute(value, (axis, "c"), pairs)


def ring_pieces(pack, axis, n):
    p = [pack]
    for _ in range(1, n // 2):
        p.append(spread(p[-1], axis, n))
    return p, spread(p[-1][0], axis, n)


def rows_ring(pack):
    p, far = ring_pieces(pack, "y", NY)
    return [p[0], p[1], far, swapped(p[1]), swapped(far)]


Y_ORDER = (
    (0, 0, 0, 0), (0, 1, 0, 1), (1, 0, 1, 0), (1, 1, 1, 1),
    (2, None, 2, 0), (4, None, 2, 1), (3, 1, 3, 0), (3, 0, 3, 1),
)


def reduced_rows(give, keep_far, keep_next, home):
    given = swapped(give).astype(f32)
    far = (keep_far.astype(f32) + given[:OWN]).astype(bf16)
    far = spread(far, "y", NY)
    follow = keep_next.astype(f32) + given[OWN:]
    follow = jnp.concatenate([follow[:OWN] + far.astype(f32), follow[OWN:]], axis=0).astype(bf16)
    return (home.astype(f32) + spread(follow, "y", NY).astype(f32)).astype(bf16)


def gelu(v):
    return 0.5 * v * (1.0 + jnp.tanh(0.7978845608028654 * (v + 0.044715 * v * v * v)))


def one_less_exp(u):
    s = 1.0 + u * (1.0 / 8.0)
    for k in range(7, 1, -1):
        s = 1.0 + u * (1.0 / k) * s
    return jnp.where(u > -0.5, -u * s, 1.0 - jnp.exp(u))


def stretch(index, size):
    return pl.ds(pl.multiple_of(index * size, size), size)


def upstream(axis, n, k):
    sign = 1 - 2 * lax.axis_index("c")
    return lax.rem(lax.axis_index(axis) + n - k * sign, n)


def core(rel):
    return lax.axis_index("c") if rel == 0 else 1 - lax.axis_index("c")


def dot_nt(a, b):
    return lax.dot_general(a, b, (((1,), (1,)), ((), ())), preferred_element_type=f32)


def projected(hid_ref, turned_ref, wout_ref, outs):
    my = lax.axis_index("y")
    sign = 1 - 2 * lax.axis_index("c")
    ahead, behind = lax.rem(my + NY + sign, NY), lax.rem(my + NY - sign, NY)
    across = lax.rem(my + 2, NY)
    order = [
        (across, 1), (behind, 1), (behind, 0), (across, 0), (ahead, 0), (ahead, 1), (my, 0), (my, 1),
    ]
    for i, (chip, rel) in enumerate(order):
        turned_ref[i * OWN : (i + 1) * OWN, :] = hid_ref[stretch(chip * NC + core(rel), OWN), :]

    def columns(k, _):
        at = stretch(k, PIECE)
        part = dot_nt(turned_ref[...], wout_ref[at, :]).astype(bf16)
        first = 0
        for ref in outs:
            ref[:, at] = part[first : first + ref.shape[0], :]
            first += ref.shape[0]
        return 0

    lax.fori_loop(0, NTP, columns, 0)


def behind(me, by, n):
    return lax.rem(me + (n - by), n)


def laid_kernel(*refs):
    blocks, mix_ref, down_ref = refs[:NZ], refs[NZ], refs[NZ + 1]
    mz = lax.axis_index("z")
    for k in range(NZ):
        mix_ref[k] = blocks[k][:, 0:768]
        down_ref[behind(mz, k, NZ)] = blocks[k][:, 768:]


def laid(blocks):
    return pl.pallas_call(
        laid_kernel,
        out_shape=(
            jax.ShapeDtypeStruct((NZ, 64, 768), bf16), jax.ShapeDtypeStruct((NZ, 64, UNITS), bf16),
        ),
        in_specs=[VMEM] * NZ,
        out_specs=(VMEM,) * 2,
        compiler_params=pltpu.CompilerParams(vmem_limit_bytes=4 * 1024 * 1024),
        cost_estimate=pl.CostEstimate(flops=1000, bytes_accessed=3 * 1024 * 1024, transcendentals=0),
        name="laid",
    )(*blocks)


def mixer_kernel(*refs):
    x_refs, w_refs = [*refs[0:4], refs[3].at[2]], refs[4:8]
    taps_ref, recur_ref, inject_ref, slope_ref = refs[8:12]
    outs, own_ref, gain_ref = refs[12:16], refs[16], refs[17]
    v_ref, win_ref, wout_ref, gate_ref, in_ref, keep_ref, drive_ref, hid_ref, turned_ref = refs[18:]
    mz, mx = lax.axis_index("z"), lax.axis_index("x")

    def placed(kz, _):
        for kx in range(NX):
            z, x = lax.rem(mz + NZ - kz, NZ), behind(mx, kx, NX)
            at = pl.ds(pl.multiple_of((z * NX + x) * 64, 64), 64)
            win_ref[at, :] = w_refs[kx][kz, :, 0:512]
            wout_ref[at, :] = w_refs[kx][kz, :, 512:]
        return 0

    lax.fori_loop(0, NZ, placed, 0)
    xs = []
    for operand, entry, ky, rel in Y_ORDER:
        ref = x_refs[operand] if entry is None else x_refs[operand].at[entry]
        xs.append((ref, stretch(upstream("y", NY, ky) * NC + core(rel), PIECE)))
    for ref, at in xs:
        for rel in (0, 1):
            own_ref[rel * OWN : (rel + 1) * OWN, at] = ref[
                stretch(lax.axis_index("y") * NC + core(rel), OWN), :
            ]
        gain_ref[:, at] = ref[ROWS : ROWS + 8, :]

    def normed(i, _):
        rows = stretch(i, 128)
        squares = jnp.zeros((128, 1), f32)
        for ref, _at in xs:
            v = ref[rows, :].astype(f32)
            squares = squares + jnp.sum(v * v, axis=1, keepdims=True)
        factor = lax.rsqrt(squares / D + norm_eps)
        for ref, at in xs:
            gain = ref[ROWS : ROWS + 1, :].astype(f32)
            v_ref[rows, at] = (ref[rows, :].astype(f32) * factor * gain).astype(bf16)
        return 0

    lax.fori_loop(0, ROWS // 128, normed, 0)
    gate_ref[...] = jnp.dot(
        v_ref[...], win_ref[:, 0:PIECE], preferred_element_type=f32
    ).astype(bf16)
    in_ref[0:TOP, :] = jnp.zeros((TOP, PIECE), bf16)
    in_ref[TOP:, :] = jnp.dot(
        v_ref[...], win_ref[:, PIECE:], preferred_element_type=f32
    ).astype(bf16)
    taps = taps_ref[...].astype(f32)
    within = lax.broadcasted_iota(jnp.int32, (CHUNK, PIECE), 0) % 8

    def chunk(i, carry):
        first = pl.multiple_of(i * CHUNK, CHUNK)
        rows = pl.ds(first, CHUNK)
        v = in_ref[pl.ds(first, CHUNK + TOP), :].astype(f32)
        smoothed = v[TOP:] * taps[3:4, :]
        for back in (1, 2, 3):
            smoothed = smoothed + pltpu.roll(v, back, 0)[TOP:] * taps[3 - back : 4 - back, :]
        smoothed = smoothed.astype(bf16)
        recur = jax.nn.sigmoid(jnp.dot(smoothed, recur_ref[...], preferred_element_type=f32))
        inject = jax.nn.sigmoid(jnp.dot(smoothed, inject_ref[...], preferred_element_type=f32))
        log_retain = -gate_power * recur * slope_ref[...]
        keep = jnp.exp(log_retain)
        drive = jnp.sqrt(one_less_exp(2.0 * log_retain)) * inject * smoothed.astype(f32)
        for by in (1, 2, 4):
            ok = within >= by
            drive = jnp.where(ok, keep * pltpu.roll(drive, by, 0), 0.0) + drive
            keep = jnp.where(ok, pltpu.roll(keep, by, 0), 1.0) * keep
        keep_ref[...] = keep
        drive_ref[...] = drive
        for t in range(CHUNK // 8):
            at = slice(8 * t, 8 * t + 8)
            state = keep_ref[at, :] * carry + drive_ref[at, :]
            drive_ref[at, :] = state
            carry = state[7:8, :]
        hid_ref[rows, :] = (gelu(gate_ref[rows, :].astype(f32)) * drive_ref[...]).astype(bf16)
        return carry

    lax.fori_loop(0, ROWS // CHUNK, chunk, jnp.zeros((1, PIECE), f32))
    projected(hid_ref, turned_ref, wout_ref, outs)


CHUNK = 256
TOP = 16
VMEM = pl.BlockSpec(memory_space=pltpu.VMEM)
PARTS = tuple(jax.ShapeDtypeStruct((n * OWN, D), bf16) for n in (3, 1, 2, 2))
PAIR = jax.ShapeDtypeStruct((2 * OWN, D), bf16)


def mixer(operands):
    return pl.pallas_call(
        mixer_kernel,
        out_shape=(*PARTS, PAIR, jax.ShapeDtypeStruct((8, D), bf16)),
        in_specs=[VMEM] * len(operands),
        out_specs=(VMEM,) * 6,
        scratch_shapes=[
            pltpu.VMEM((ROWS, D), bf16),
            pltpu.VMEM((D, 512), bf16),
            pltpu.VMEM((D, PIECE), bf16),
            pltpu.VMEM((ROWS, PIECE), bf16),
            pltpu.VMEM((ROWS + TOP, PIECE), bf16),
            pltpu.VMEM((CHUNK, PIECE), f32),
            pltpu.VMEM((CHUNK, PIECE), f32),
            pltpu.VMEM((ROWS, PIECE), bf16),
            pltpu.VMEM((ROWS, PIECE), bf16),
        ],
        compiler_params=pltpu.CompilerParams(vmem_limit_bytes=14 * 1024 * 1024),
        cost_estimate=pl.CostEstimate(
            flops=2 * ROWS * D * 768 + 4 * ROWS * PIECE * PIECE,
            bytes_accessed=8 * 1024 * 1024, transcendentals=ROWS * PIECE * 6,
        ),
        name="mixer",
    )(*operands)


def row_normed(widened, row_gain):
    factor = lax.rsqrt(jnp.sum(widened * widened, axis=1, keepdims=True) / D + norm_eps)
    return widened * factor * row_gain.astype(f32)


UP_CUT = 256
UP_CUTS = 6


def ffn_kernel(*refs):
    n_refs, up_w, down_w, taps_ref = refs[0:5], refs[5], refs[6], refs[7]
    outs = refs[8:12]
    n_all, up_ref, act_ref, turned_ref = refs[12:]
    for operand, entry, ky, rel in Y_ORDER:
        ref = n_refs[operand] if entry is None else n_refs[operand].at[entry]
        n_all[stretch(upstream("y", NY, ky) * NC + core(rel), OWN), :] = ref[...]
    up_ref[0:TOP, :] = jnp.zeros((TOP, 2 * UNITS), bf16)

    def up(at):
        up_ref[TOP:, at] = jnp.dot(
            n_all[...], up_w[:, at], preferred_element_type=f32
        ).astype(bf16)

    def loop(i, _):
        up(stretch(i, UP_CUT))
        return 0

    lax.fori_loop(0, UP_CUTS - 1, loop, 0)
    up(pl.ds((UP_CUTS - 1) * UP_CUT, 128))
    taps = taps_ref[...].astype(f32)

    def smooth(i, _):
        at = pl.multiple_of(i * 64, 64)
        v = up_ref[pl.ds(at, 64 + TOP), :].astype(f32)
        conv = v[TOP:] * taps[2:3, :]
        for back in (1, 2):
            conv = conv + pltpu.roll(v, back, 0)[TOP:] * taps[2 - back : 3 - back, :]
        act_ref[pl.ds(at, 64), :] = (gelu(conv[:, 0:UNITS]) * conv[:, UNITS:]).astype(bf16)
        return 0

    lax.fori_loop(0, ROWS // 64, smooth, 0)
    projected(act_ref, turned_ref, down_w, outs)


def ffn(operands):
    return pl.pallas_call(
        ffn_kernel,
        out_shape=PARTS,
        in_specs=[VMEM] * 8,
        out_specs=(VMEM,) * 4,
        scratch_shapes=[
            pltpu.VMEM((ROWS, D), bf16),
            pltpu.VMEM((ROWS + TOP, 2 * UNITS), bf16),
            pltpu.VMEM((ROWS, UNITS), bf16),
            pltpu.VMEM((ROWS, UNITS), bf16),
        ],
        compiler_params=pltpu.CompilerParams(vmem_limit_bytes=14 * 1024 * 1024),
        cost_estimate=pl.CostEstimate(
            flops=2 * ROWS * D * 3 * UNITS, bytes_accessed=13 * 1024 * 1024,
            transcendentals=ROWS * UNITS,
        ),
        name="ffn",
    )(*operands)


def shards(
    tokens, pre_mix_gain, w_gate_in, w_input, mix_kernel, w_recur, w_inject, decay_param,
    w_mix_out, post_mix_gain, pre_ffn_gain, w_up_gate, w_up_value, gate_kernel, value_kernel,
    w_down, post_ffn_gain,
):
    z_own = jnp.concatenate([w_gate_in, w_input, w_mix_out.T, w_down.T], axis=1)
    along_z = ring_gathered(z_own, "z", NZ)
    gains = jnp.concatenate([pre_mix_gain, post_mix_gain, pre_ffn_gain, post_ffn_gain])
    gains = gains.reshape(4, PIECE)
    packed = jnp.concatenate([tokens, jnp.pad(gains, ((0, EXTRA - 4), (0, 0)))], axis=0)
    mix_z, down_z = laid(along_z)
    mix_blocks = ring_gathered(mix_z, "x", NX)
    packed = jnp.stack([packed, swapped(packed)])
    p, far = ring_pieces(packed, "y", NY)
    x_blocks = [*p, far, swapped(jnp.concatenate([p[1], far[None]], axis=0))]
    up_own = jnp.concatenate([w_up_gate, w_up_value], axis=1)
    sent = jnp.broadcast_to(up_own[None], (NX, *up_own.shape))
    along_x = lax.all_to_all(sent, "x", 0, 0, tiled=True)
    up_all = in_order(ring_gathered(along_x, "z", NZ), "z", 0).reshape(D, 2 * UNITS)
    down_all = in_order(ring_gathered(down_z, "x", NX), "x", 1).reshape(D, UNITS)
    x_blocks[1], decay_param = lax.optimization_barrier((x_blocks[1], decay_param))
    slope = jax.nn.softplus(-decay_param)[None, :]
    *parts, own_rows, gain_rows = mixer(
        (*x_blocks, *mix_blocks, mix_kernel, w_recur[0], w_inject[0], slope)
    )
    part = reduced_rows(*parts)
    part, taps_of = lax.optimization_barrier((part, (gate_kernel, value_kernel)))
    taps = jnp.concatenate(taps_of, axis=1)
    turned = swapped(jnp.concatenate([part[OWN:], part[:OWN]], axis=0))
    mixer_sum = part.astype(f32) + turned.astype(f32)
    middle = (own_rows.astype(f32) + row_normed(mixer_sum, gain_rows[1:2])).astype(bf16)
    normed = row_normed(middle.astype(f32), gain_rows[2:3]).astype(bf16).reshape(2, OWN, D)
    parts = ffn((*rows_ring(normed), up_all, down_all, taps))
    part = reduced_rows(*parts)
    ffn_sum = part[:OWN].astype(f32) + swapped(part[OWN:]).astype(f32)
    out_rows = middle[:OWN].astype(f32) + row_normed(ffn_sum, gain_rows[3:4])
    to_columns = out_rows.astype(bf16).reshape(OWN, NTP, PIECE).transpose(1, 0, 2)
    return lax.all_to_all(to_columns, TP, 0, 0, tiled=True).reshape(ROWS, PIECE)


def solution(mesh):
    finer = Mesh(mesh.devices.reshape(NZ, NX, NY, NC), ("z", "x", "y", "c"))
    return jax.shard_map(
        shards,
        mesh=finer,
        in_specs=(
            P(FS, TP), P(TP), P(FS, TP), P(FS, TP), P(None, TP), P(TP, None, None),
            P(TP, None, None), P(TP), P(TP, FS), P(TP), P(TP), P(FS, TP), P(FS, TP),
            P(None, TP), P(None, TP), P(TP, FS), P(TP),
        ),
        out_specs=P(FS, TP),
        check_vma=False,
    )
```

```python
import jax
import jax.numpy as jnp
from jax import lax
from jax.experimental import pallas as pl
from jax.experimental.pallas import tpu as pltpu
from jax.sharding import Mesh
from jax.sharding import PartitionSpec as P


D = 2048
FS = ("z", "x")
TP = ("y", "c")
NZ, NX, NY, NC = 8, 4, 4, 2
NTP = NY * NC
ROWS = 512
OWN = ROWS // NTP
PIECE = D // NTP
EXTRA = 16
UNITS = 704
norm_eps = 1e-06
gate_power = 8.0
bf16, f32 = jnp.bfloat16, jnp.float32


def moved(value, axis, n, by):
    return lax.ppermute(value, axis, [(i, (i + by) % n) for i in range(n)])


def ring_gathered(block, axis, n):
    got = [block] + [None] * (n - 1)
    ahead = back = block
    for s in range(1, n // 2):
        ahead = moved(ahead, axis, n, 1)
        back = moved(back, axis, n, -1)
        got[s], got[n - s] = ahead, back
    far = jnp.where(lax.axis_index("c") == 0, ahead, back)
    got[n // 2] = spread(far, axis, n)
    return got


def in_order(blocks, axis, dim):
    n, me = len(blocks), lax.axis_index(axis)
    shape = blocks[0].shape
    whole = jnp.zeros((*shape[:dim], n, *shape[dim:]), blocks[0].dtype)
    order = [k for j in range(1, n // 2) for k in (j, n - j)] + [n // 2]
    for k in [1, 0, *order[1:]]:
        start = [0] * whole.ndim
        start[dim] = lax.rem(me + (n - k), n)
        whole = lax.dynamic_update_slice(whole, jnp.expand_dims(blocks[k], dim), start)
    return whole


def swapped(value):
    return lax.ppermute(value, "c", [(0, 1), (1, 0)])


def spread(value, axis, n):
    pairs = [(2 * i, 2 * ((i + 1) % n)) for i in range(n)]
    pairs += [(2 * i + 1, 2 * ((i - 1) % n) + 1) for i in range(n)]
    return lax.ppermute(value, (axis, "c"), pairs)


def ring_pieces(pack, axis, n):
    p = [pack]
    for _ in range(1, n // 2):
        p.append(spread(p[-1], axis, n))
    return p, spread(p[-1][0], axis, n)


def rows_ring(pack):
    p, far = ring_pieces(pack, "y", NY)
    return [p[0], p[1], far, swapped(p[1]), swapped(far)]


Y_ORDER = (
    (0, 0, 0, 0), (0, 1, 0, 1), (1, 0, 1, 0), (1, 1, 1, 1),
    (2, None, 2, 0), (4, None, 2, 1), (3, 1, 3, 0), (3, 0, 3, 1),
)


def reduced_rows(give, keep_far, keep_next, home):
    given = swapped(give).astype(f32)
    far = (keep_far.astype(f32) + given[:OWN]).astype(bf16)
    far = spread(far, "y", NY)
    follow = keep_next.astype(f32) + given[OWN:]
    follow = jnp.concatenate([follow[:OWN] + far.astype(f32), follow[OWN:]], axis=0).astype(bf16)
    return (home.astype(f32) + spread(follow, "y", NY).astype(f32)).astype(bf16)


def gelu(v):
    return 0.5 * v * (1.0 + jnp.tanh(0.7978845608028654 * (v + 0.044715 * v * v * v)))


def one_less_exp(u):
    s = 1.0 + u * (1.0 / 8.0)
    for k in range(7, 1, -1):
        s = 1.0 + u * (1.0 / k) * s
    return jnp.where(u > -0.5, -u * s, 1.0 - jnp.exp(u))


def stretch(index, size):
    return pl.ds(pl.multiple_of(index * size, size), size)


def upstream(axis, n, k):
    sign = 1 - 2 * lax.axis_index("c")
    return lax.rem(lax.axis_index(axis) + n - k * sign, n)


def core(rel):
    return lax.axis_index("c") if rel == 0 else 1 - lax.axis_index("c")


def dot_nt(a, b):
    return lax.dot_general(a, b, (((1,), (1,)), ((), ())), preferred_element_type=f32)


def projected(hid_ref, turned_ref, wout_ref, outs):
    my = lax.axis_index("y")
    sign = 1 - 2 * lax.axis_index("c")
    ahead, behind = lax.rem(my + NY + sign, NY), lax.rem(my + NY - sign, NY)
    across = lax.rem(my + 2, NY)
    order = [
        (across, 1), (behind, 1), (behind, 0), (across, 0), (ahead, 0), (ahead, 1), (my, 0), (my, 1),
    ]
    for i, (chip, rel) in enumerate(order):
        turned_ref[i * OWN : (i + 1) * OWN, :] = hid_ref[stretch(chip * NC + core(rel), OWN), :]

    def columns(k, _):
        at = stretch(k, PIECE)
        part = dot_nt(turned_ref[...], wout_ref[at, :]).astype(bf16)
        first = 0
        for ref in outs:
            ref[:, at] = part[first : first + ref.shape[0], :]
            first += ref.shape[0]
        return 0

    lax.fori_loop(0, NTP, columns, 0)


def behind(me, by, n):
    return lax.rem(me + (n - by), n)


def laid_kernel(*refs):
    blocks, mix_ref, down_ref = refs[:NZ], refs[NZ], refs[NZ + 1]
    mz = lax.axis_index("z")
    for k in range(NZ):
        mix_ref[k] = blocks[k][:, 0:768]
        down_ref[behind(mz, k, NZ)] = blocks[k][:, 768:]


def laid(blocks):
    return pl.pallas_call(
        laid_kernel,
        out_shape=(
            jax.ShapeDtypeStruct((NZ, 64, 768), bf16), jax.ShapeDtypeStruct((NZ, 64, UNITS), bf16),
        ),
        in_specs=[VMEM] * NZ,
        out_specs=(VMEM,) * 2,
        compiler_params=pltpu.CompilerParams(vmem_limit_bytes=4 * 1024 * 1024),
        cost_estimate=pl.CostEstimate(flops=1000, bytes_accessed=3 * 1024 * 1024, transcendentals=0),
        name="laid",
    )(*blocks)


def mixer_kernel(*refs):
    x_refs, w_refs = refs[0:5], refs[5:9]
    taps_ref, recur_ref, inject_ref, slope_ref = refs[9:13]
    outs, own_ref, gain_ref = refs[13:17], refs[17], refs[18]
    v_ref, win_ref, wout_ref, gate_ref, in_ref, keep_ref, drive_ref, hid_ref, turned_ref = refs[19:]
    mz, mx = lax.axis_index("z"), lax.axis_index("x")

    def placed(kz, _):
        for kx in range(NX):
            z, x = lax.rem(mz + NZ - kz, NZ), behind(mx, kx, NX)
            at = pl.ds(pl.multiple_of((z * NX + x) * 64, 64), 64)
            win_ref[at, :] = w_refs[kx][kz, :, 0:512]
            wout_ref[at, :] = w_refs[kx][kz, :, 512:]
        return 0

    lax.fori_loop(0, NZ, placed, 0)
    xs = []
    for operand, entry, ky, rel in Y_ORDER:
        ref = x_refs[operand] if entry is None else x_refs[operand].at[entry]
        xs.append((ref, stretch(upstream("y", NY, ky) * NC + core(rel), PIECE)))
    for ref, at in xs:
        for rel in (0, 1):
            own_ref[rel * OWN : (rel + 1) * OWN, at] = ref[
                stretch(lax.axis_index("y") * NC + core(rel), OWN), :
            ]
        gain_ref[:, at] = ref[ROWS : ROWS + 8, :]

    def normed(i, _):
        rows = stretch(i, 128)
        squares = jnp.zeros((128, 1), f32)
        for ref, _at in xs:
            v = ref[rows, :].astype(f32)
            squares = squares + jnp.sum(v * v, axis=1, keepdims=True)
        factor = lax.rsqrt(squares / D + norm_eps)
        for ref, at in xs:
            gain = ref[ROWS : ROWS + 1, :].astype(f32)
            v_ref[rows, at] = (ref[rows, :].astype(f32) * factor * gain).astype(bf16)
        return 0

    lax.fori_loop(0, ROWS // 128, normed, 0)
    gate_ref[...] = jnp.dot(
        v_ref[...], win_ref[:, 0:PIECE], preferred_element_type=f32
    ).astype(bf16)
    in_ref[0:TOP, :] = jnp.zeros((TOP, PIECE), bf16)
    in_ref[TOP:, :] = jnp.dot(
        v_ref[...], win_ref[:, PIECE:], preferred_element_type=f32
    ).astype(bf16)
    taps = taps_ref[...].astype(f32)
    within = lax.broadcasted_iota(jnp.int32, (CHUNK, PIECE), 0) % 8

    def chunk(i, carry):
        first = pl.multiple_of(i * CHUNK, CHUNK)
        rows = pl.ds(first, CHUNK)
        v = in_ref[pl.ds(first, CHUNK + TOP), :].astype(f32)
        smoothed = v[TOP:] * taps[3:4, :]
        for back in (1, 2, 3):
            smoothed = smoothed + pltpu.roll(v, back, 0)[TOP:] * taps[3 - back : 4 - back, :]
        smoothed = smoothed.astype(bf16)
        recur = jax.nn.sigmoid(jnp.dot(smoothed, recur_ref[...], preferred_element_type=f32))
        inject = jax.nn.sigmoid(jnp.dot(smoothed, inject_ref[...], preferred_element_type=f32))
        log_retain = -gate_power * recur * slope_ref[...]
        keep = jnp.exp(log_retain)
        drive = jnp.sqrt(one_less_exp(2.0 * log_retain)) * inject * smoothed.astype(f32)
        for by in (1, 2, 4):
            ok = within >= by
            drive = jnp.where(ok, keep * pltpu.roll(drive, by, 0), 0.0) + drive
            keep = jnp.where(ok, pltpu.roll(keep, by, 0), 1.0) * keep
        keep_ref[...] = keep
        drive_ref[...] = drive
        for t in range(CHUNK // 8):
            at = slice(8 * t, 8 * t + 8)
            state = keep_ref[at, :] * carry + drive_ref[at, :]
            drive_ref[at, :] = state
            carry = state[7:8, :]
        hid_ref[rows, :] = (gelu(gate_ref[rows, :].astype(f32)) * drive_ref[...]).astype(bf16)
        return carry

    lax.fori_loop(0, ROWS // CHUNK, chunk, jnp.zeros((1, PIECE), f32))
    projected(hid_ref, turned_ref, wout_ref, outs)


CHUNK = 128
TOP = 16
VMEM = pl.BlockSpec(memory_space=pltpu.VMEM)
PARTS = tuple(jax.ShapeDtypeStruct((n * OWN, D), bf16) for n in (3, 1, 2, 2))
PAIR = jax.ShapeDtypeStruct((2 * OWN, D), bf16)


def mixer(operands):
    return pl.pallas_call(
        mixer_kernel,
        out_shape=(*PARTS, PAIR, jax.ShapeDtypeStruct((8, D), bf16)),
        in_specs=[VMEM] * len(operands),
        out_specs=(VMEM,) * 6,
        scratch_shapes=[
            pltpu.VMEM((ROWS, D), bf16),
            pltpu.VMEM((D, 512), bf16),
            pltpu.VMEM((D, PIECE), bf16),
            pltpu.VMEM((ROWS, PIECE), bf16),
            pltpu.VMEM((ROWS + TOP, PIECE), bf16),
            pltpu.VMEM((CHUNK, PIECE), f32),
            pltpu.VMEM((CHUNK, PIECE), f32),
            pltpu.VMEM((ROWS, PIECE), bf16),
            pltpu.VMEM((ROWS, PIECE), bf16),
        ],
        compiler_params=pltpu.CompilerParams(vmem_limit_bytes=14 * 1024 * 1024),
        cost_estimate=pl.CostEstimate(
            flops=2 * ROWS * D * 768 + 4 * ROWS * PIECE * PIECE,
            bytes_accessed=8 * 1024 * 1024, transcendentals=ROWS * PIECE * 6,
        ),
        name="mixer",
    )(*operands)


def row_normed(widened, row_gain):
    factor = lax.rsqrt(jnp.sum(widened * widened, axis=1, keepdims=True) / D + norm_eps)
    return widened * factor * row_gain.astype(f32)


UP_CUT = 256
UP_CUTS = 6


def ffn_kernel(*refs):
    n_refs, up_w, down_w, taps_ref = refs[0:5], refs[5], refs[6], refs[7]
    outs = refs[8:12]
    n_all, up_ref, act_ref, turned_ref = refs[12:]
    for operand, entry, ky, rel in Y_ORDER:
        ref = n_refs[operand] if entry is None else n_refs[operand].at[entry]
        n_all[stretch(upstream("y", NY, ky) * NC + core(rel), OWN), :] = ref[...]
    up_ref[0:TOP, :] = jnp.zeros((TOP, 2 * UNITS), bf16)

    def up(at):
        up_ref[TOP:, at] = jnp.dot(
            n_all[...], up_w[:, at], preferred_element_type=f32
        ).astype(bf16)

    def loop(i, _):
        up(stretch(i, UP_CUT))
        return 0

    lax.fori_loop(0, UP_CUTS - 1, loop, 0)
    up(pl.ds((UP_CUTS - 1) * UP_CUT, 128))
    taps = taps_ref[...].astype(f32)

    def smooth(i, _):
        at = pl.multiple_of(i * 64, 64)
        v = up_ref[pl.ds(at, 64 + TOP), :].astype(f32)
        conv = v[TOP:] * taps[2:3, :]
        for back in (1, 2):
            conv = conv + pltpu.roll(v, back, 0)[TOP:] * taps[2 - back : 3 - back, :]
        act_ref[pl.ds(at, 64), :] = (gelu(conv[:, 0:UNITS]) * conv[:, UNITS:]).astype(bf16)
        return 0

    lax.fori_loop(0, ROWS // 64, smooth, 0)
    projected(act_ref, turned_ref, down_w, outs)


def ffn(operands):
    return pl.pallas_call(
        ffn_kernel,
        out_shape=PARTS,
        in_specs=[VMEM] * 8,
        out_specs=(VMEM,) * 4,
        scratch_shapes=[
            pltpu.VMEM((ROWS, D), bf16),
            pltpu.VMEM((ROWS + TOP, 2 * UNITS), bf16),
            pltpu.VMEM((ROWS, UNITS), bf16),
            pltpu.VMEM((ROWS, UNITS), bf16),
        ],
        compiler_params=pltpu.CompilerParams(vmem_limit_bytes=14 * 1024 * 1024),
        cost_estimate=pl.CostEstimate(
            flops=2 * ROWS * D * 3 * UNITS, bytes_accessed=13 * 1024 * 1024,
            transcendentals=ROWS * UNITS,
        ),
        name="ffn",
    )(*operands)


def shards(
    tokens, pre_mix_gain, w_gate_in, w_input, mix_kernel, w_recur, w_inject, decay_param,
    w_mix_out, post_mix_gain, pre_ffn_gain, w_up_gate, w_up_value, gate_kernel, value_kernel,
    w_down, post_ffn_gain,
):
    z_own = jnp.concatenate([w_gate_in, w_input, w_mix_out.T, w_down.T], axis=1)
    along_z = ring_gathered(z_own, "z", NZ)
    gains = jnp.concatenate([pre_mix_gain, post_mix_gain, pre_ffn_gain, post_ffn_gain])
    gains = gains.reshape(4, PIECE)
    packed = jnp.concatenate([tokens, jnp.pad(gains, ((0, EXTRA - 4), (0, 0)))], axis=0)
    mix_z, down_z = laid(along_z)
    mix_blocks = ring_gathered(mix_z, "x", NX)
    packed = jnp.stack([packed, swapped(packed)])
    x_blocks = rows_ring(packed)
    up_own = jnp.concatenate([w_up_gate, w_up_value], axis=1)
    sent = jnp.broadcast_to(up_own[None], (NX, *up_own.shape))
    along_x = lax.all_to_all(sent, "x", 0, 0, tiled=True)
    up_all = in_order(ring_gathered(along_x, "z", NZ), "z", 0).reshape(D, 2 * UNITS)
    down_all = in_order(ring_gathered(down_z, "x", NX), "x", 1).reshape(D, UNITS)
    x_blocks[1], decay_param = lax.optimization_barrier((x_blocks[1], decay_param))
    slope = jax.nn.softplus(-decay_param)[None, :]
    *parts, own_rows, gain_rows = mixer(
        (*x_blocks, *mix_blocks, mix_kernel, w_recur[0], w_inject[0], slope)
    )
    part = reduced_rows(*parts)
    part, taps_of = lax.optimization_barrier((part, (gate_kernel, value_kernel)))
    taps = jnp.concatenate(taps_of, axis=1)
    turned = swapped(jnp.concatenate([part[OWN:], part[:OWN]], axis=0))
    mixer_sum = part.astype(f32) + turned.astype(f32)
    middle = (own_rows.astype(f32) + row_normed(mixer_sum, gain_rows[1:2])).astype(bf16)
    normed = row_normed(middle.astype(f32), gain_rows[2:3]).astype(bf16).reshape(2, OWN, D)
    parts = ffn((*rows_ring(normed), up_all, down_all, taps))
    part = reduced_rows(*parts)
    ffn_sum = part[:OWN].astype(f32) + swapped(part[OWN:]).astype(f32)
    out_rows = middle[:OWN].astype(f32) + row_normed(ffn_sum, gain_rows[3:4])
    to_columns = out_rows.astype(bf16).reshape(OWN, NTP, PIECE).transpose(1, 0, 2)
    return lax.all_to_all(to_columns, TP, 0, 0, tiled=True).reshape(ROWS, PIECE)


def solution(mesh):
    finer = Mesh(mesh.devices.reshape(NZ, NX, NY, NC), ("z", "x", "y", "c"))
    return jax.shard_map(
        shards,
        mesh=finer,
        in_specs=(
            P(FS, TP), P(TP), P(FS, TP), P(FS, TP), P(None, TP), P(TP, None, None),
            P(TP, None, None), P(TP), P(TP, FS), P(TP), P(TP), P(FS, TP), P(FS, TP),
            P(None, TP), P(None, TP), P(TP, FS), P(TP),
        ),
        out_specs=P(FS, TP),
        check_vma=False,
    )
```

```python
import jax
import jax.numpy as jnp
from jax import lax
from jax.experimental import pallas as pl
from jax.experimental.pallas import tpu as pltpu
from jax.sharding import Mesh
from jax.sharding import PartitionSpec as P


D = 2048
FS = ("z", "x")
TP = ("y", "c")
NZ, NX, NY, NC = 8, 4, 4, 2
NTP = NY * NC
ROWS = 512
OWN = ROWS // NTP
PIECE = D // NTP
EXTRA = 16
UNITS = 704
norm_eps = 1e-06
gate_power = 8.0
bf16, f32 = jnp.bfloat16, jnp.float32


def moved(value, axis, n, by):
    return lax.ppermute(value, axis, [(i, (i + by) % n) for i in range(n)])


def ring_gathered(block, axis, n):
    got = [block] + [None] * (n - 1)
    ahead = back = block
    for s in range(1, n // 2):
        ahead = moved(ahead, axis, n, 1)
        back = moved(back, axis, n, -1)
        got[s], got[n - s] = ahead, back
    far = jnp.where(lax.axis_index("c") == 0, ahead, back)
    got[n // 2] = spread(far, axis, n)
    return got


def in_order(blocks, axis, dim):
    n, me = len(blocks), lax.axis_index(axis)
    shape = blocks[0].shape
    whole = jnp.zeros((*shape[:dim], n, *shape[dim:]), blocks[0].dtype)
    order = [k for j in range(1, n // 2) for k in (j, n - j)] + [n // 2]
    for k in [1, 0, *order[1:]]:
        start = [0] * whole.ndim
        start[dim] = lax.rem(me + (n - k), n)
        whole = lax.dynamic_update_slice(whole, jnp.expand_dims(blocks[k], dim), start)
    return whole


def swapped(value):
    return lax.ppermute(value, "c", [(0, 1), (1, 0)])


def spread(value, axis, n):
    pairs = [(2 * i, 2 * ((i + 1) % n)) for i in range(n)]
    pairs += [(2 * i + 1, 2 * ((i - 1) % n) + 1) for i in range(n)]
    return lax.ppermute(value, (axis, "c"), pairs)


def ring_pieces(pack, axis, n):
    p = [pack]
    for _ in range(1, n // 2):
        p.append(spread(p[-1], axis, n))
    return p, spread(p[-1][0], axis, n)


def rows_ring(pack):
    p, far = ring_pieces(pack, "y", NY)
    return [p[0], p[1], far, swapped(p[1]), swapped(far)]


Y_ORDER = (
    (0, 0, 0, 0), (0, 1, 0, 1), (1, 0, 1, 0), (1, 1, 1, 1),
    (2, None, 2, 0), (4, None, 2, 1), (3, 1, 3, 0), (3, 0, 3, 1),
)


def reduced_rows(give, keep_far, keep_next, home):
    given = swapped(give).astype(f32)
    far = (keep_far.astype(f32) + given[:OWN]).astype(bf16)
    far = spread(far, "y", NY)
    follow = keep_next.astype(f32) + given[OWN:]
    follow = jnp.concatenate([follow[:OWN] + far.astype(f32), follow[OWN:]], axis=0).astype(bf16)
    return (home.astype(f32) + spread(follow, "y", NY).astype(f32)).astype(bf16)


def gelu(v):
    return 0.5 * v * (1.0 + jnp.tanh(0.7978845608028654 * (v + 0.044715 * v * v * v)))


def one_less_exp(u):
    s = 1.0 + u * (1.0 / 8.0)
    for k in range(7, 1, -1):
        s = 1.0 + u * (1.0 / k) * s
    return jnp.where(u > -0.5, -u * s, 1.0 - jnp.exp(u))


def stretch(index, size):
    return pl.ds(pl.multiple_of(index * size, size), size)


def upstream(axis, n, k):
    sign = 1 - 2 * lax.axis_index("c")
    return lax.rem(lax.axis_index(axis) + n - k * sign, n)


def core(rel):
    return lax.axis_index("c") if rel == 0 else 1 - lax.axis_index("c")


def dot_nt(a, b):
    return lax.dot_general(a, b, (((1,), (1,)), ((), ())), preferred_element_type=f32)


def projected(hid_ref, turned_ref, wout_ref, outs):
    my = lax.axis_index("y")
    sign = 1 - 2 * lax.axis_index("c")
    ahead, behind = lax.rem(my + NY + sign, NY), lax.rem(my + NY - sign, NY)
    across = lax.rem(my + 2, NY)
    order = [
        (across, 1), (behind, 1), (behind, 0), (across, 0), (ahead, 0), (ahead, 1), (my, 0), (my, 1),
    ]
    for i, (chip, rel) in enumerate(order):
        turned_ref[i * OWN : (i + 1) * OWN, :] = hid_ref[stretch(chip * NC + core(rel), OWN), :]

    def columns(k, _):
        at = stretch(k, PIECE)
        part = dot_nt(turned_ref[...], wout_ref[at, :]).astype(bf16)
        first = 0
        for ref in outs:
            ref[:, at] = part[first : first + ref.shape[0], :]
            first += ref.shape[0]
        return 0

    lax.fori_loop(0, NTP, columns, 0)


def behind(me, by, n):
    return lax.rem(me + (n - by), n)


def laid_kernel(*refs):
    blocks, mix_ref, down_ref = refs[:NZ], refs[NZ], refs[NZ + 1]
    mz = lax.axis_index("z")
    for k in range(NZ):
        mix_ref[k] = blocks[k][:, 0:768]
        down_ref[behind(mz, k, NZ)] = blocks[k][:, 768:]


def laid(blocks):
    return pl.pallas_call(
        laid_kernel,
        out_shape=(
            jax.ShapeDtypeStruct((NZ, 64, 768), bf16), jax.ShapeDtypeStruct((NZ, 64, UNITS), bf16),
        ),
        in_specs=[VMEM] * NZ,
        out_specs=(VMEM,) * 2,
        compiler_params=pltpu.CompilerParams(vmem_limit_bytes=4 * 1024 * 1024),
        cost_estimate=pl.CostEstimate(flops=1000, bytes_accessed=3 * 1024 * 1024, transcendentals=0),
        name="laid",
    )(*blocks)


def mixer_kernel(*refs):
    x_refs, w_refs = refs[0:5], refs[5:9]
    taps_ref, recur_ref, inject_ref, slope_ref = refs[9:13]
    outs, own_ref, gain_ref = refs[13:17], refs[17], refs[18]
    v_ref, win_ref, wout_ref, gate_ref, in_ref, keep_ref, drive_ref, hid_ref, turned_ref = refs[19:]
    mz, mx = lax.axis_index("z"), lax.axis_index("x")

    def placed(kz, _):
        for kx in range(NX):
            z, x = lax.rem(mz + NZ - kz, NZ), behind(mx, kx, NX)
            at = pl.ds(pl.multiple_of((z * NX + x) * 64, 64), 64)
            win_ref[at, :] = w_refs[kx][kz, :, 0:512]
            wout_ref[at, :] = w_refs[kx][kz, :, 512:]
        return 0

    lax.fori_loop(0, NZ, placed, 0)
    xs = []
    for operand, entry, ky, rel in Y_ORDER:
        ref = x_refs[operand] if entry is None else x_refs[operand].at[entry]
        xs.append((ref, stretch(upstream("y", NY, ky) * NC + core(rel), PIECE)))
    for ref, at in xs:
        for rel in (0, 1):
            own_ref[rel * OWN : (rel + 1) * OWN, at] = ref[
                stretch(lax.axis_index("y") * NC + core(rel), OWN), :
            ]
        gain_ref[:, at] = ref[ROWS : ROWS + 8, :]

    def normed(i, _):
        rows = stretch(i, 64)
        squares = jnp.zeros((64, 1), f32)
        for ref, _at in xs:
            v = ref[rows, :].astype(f32)
            squares = squares + jnp.sum(v * v, axis=1, keepdims=True)
        factor = lax.rsqrt(squares / D + norm_eps)
        for ref, at in xs:
            gain = ref[ROWS : ROWS + 1, :].astype(f32)
            v_ref[rows, at] = (ref[rows, :].astype(f32) * factor * gain).astype(bf16)
        return 0

    lax.fori_loop(0, ROWS // 64, normed, 0)
    gate_ref[...] = jnp.dot(
        v_ref[...], win_ref[:, 0:PIECE], preferred_element_type=f32
    ).astype(bf16)
    in_ref[0:TOP, :] = jnp.zeros((TOP, PIECE), bf16)
    in_ref[TOP:, :] = jnp.dot(
        v_ref[...], win_ref[:, PIECE:], preferred_element_type=f32
    ).astype(bf16)
    taps = taps_ref[...].astype(f32)
    within = lax.broadcasted_iota(jnp.int32, (CHUNK, PIECE), 0) % 8

    def chunk(i, carry):
        first = pl.multiple_of(i * CHUNK, CHUNK)
        rows = pl.ds(first, CHUNK)
        v = in_ref[pl.ds(first, CHUNK + TOP), :].astype(f32)
        smoothed = v[TOP:] * taps[3:4, :]
        for back in (1, 2, 3):
            smoothed = smoothed + pltpu.roll(v, back, 0)[TOP:] * taps[3 - back : 4 - back, :]
        smoothed = smoothed.astype(bf16)
        recur = jax.nn.sigmoid(jnp.dot(smoothed, recur_ref[...], preferred_element_type=f32))
        inject = jax.nn.sigmoid(jnp.dot(smoothed, inject_ref[...], preferred_element_type=f32))
        log_retain = -gate_power * recur * slope_ref[...]
        keep = jnp.exp(log_retain)
        drive = jnp.sqrt(one_less_exp(2.0 * log_retain)) * inject * smoothed.astype(f32)
        for by in (1, 2, 4):
            ok = within >= by
            drive = jnp.where(ok, keep * pltpu.roll(drive, by, 0), 0.0) + drive
            keep = jnp.where(ok, pltpu.roll(keep, by, 0), 1.0) * keep
        keep_ref[...] = keep
        drive_ref[...] = drive
        for t in range(CHUNK // 8):
            at = slice(8 * t, 8 * t + 8)
            state = keep_ref[at, :] * carry + drive_ref[at, :]
            drive_ref[at, :] = state
            carry = state[7:8, :]
        hid_ref[rows, :] = (gelu(gate_ref[rows, :].astype(f32)) * drive_ref[...]).astype(bf16)
        return carry

    lax.fori_loop(0, ROWS // CHUNK, chunk, jnp.zeros((1, PIECE), f32))
    projected(hid_ref, turned_ref, wout_ref, outs)


CHUNK = 256
TOP = 16
VMEM = pl.BlockSpec(memory_space=pltpu.VMEM)
PARTS = tuple(jax.ShapeDtypeStruct((n * OWN, D), bf16) for n in (3, 1, 2, 2))
PAIR = jax.ShapeDtypeStruct((2 * OWN, D), bf16)


def mixer(operands):
    return pl.pallas_call(
        mixer_kernel,
        out_shape=(*PARTS, PAIR, jax.ShapeDtypeStruct((8, D), bf16)),
        in_specs=[VMEM] * len(operands),
        out_specs=(VMEM,) * 6,
        scratch_shapes=[
            pltpu.VMEM((ROWS, D), bf16),
            pltpu.VMEM((D, 512), bf16),
            pltpu.VMEM((D, PIECE), bf16),
            pltpu.VMEM((ROWS, PIECE), bf16),
            pltpu.VMEM((ROWS + TOP, PIECE), bf16),
            pltpu.VMEM((CHUNK, PIECE), f32),
            pltpu.VMEM((CHUNK, PIECE), f32),
            pltpu.VMEM((ROWS, PIECE), bf16),
            pltpu.VMEM((ROWS, PIECE), bf16),
        ],
        compiler_params=pltpu.CompilerParams(vmem_limit_bytes=14 * 1024 * 1024),
        cost_estimate=pl.CostEstimate(
            flops=2 * ROWS * D * 768 + 4 * ROWS * PIECE * PIECE,
            bytes_accessed=8 * 1024 * 1024, transcendentals=ROWS * PIECE * 6,
        ),
        name="mixer",
    )(*operands)


def row_normed(widened, row_gain):
    factor = lax.rsqrt(jnp.sum(widened * widened, axis=1, keepdims=True) / D + norm_eps)
    return widened * factor * row_gain.astype(f32)


UP_CUT = 256
UP_CUTS = 6


def ffn_kernel(*refs):
    n_refs, up_w, down_w, taps_ref = refs[0:5], refs[5], refs[6], refs[7]
    outs = refs[8:12]
    n_all, up_ref, act_ref, turned_ref = refs[12:]
    for operand, entry, ky, rel in Y_ORDER:
        ref = n_refs[operand] if entry is None else n_refs[operand].at[entry]
        n_all[stretch(upstream("y", NY, ky) * NC + core(rel), OWN), :] = ref[...]
    up_ref[0:TOP, :] = jnp.zeros((TOP, 2 * UNITS), bf16)

    def up(at):
        up_ref[TOP:, at] = jnp.dot(
            n_all[...], up_w[:, at], preferred_element_type=f32
        ).astype(bf16)

    def loop(i, _):
        up(stretch(i, UP_CUT))
        return 0

    lax.fori_loop(0, UP_CUTS - 1, loop, 0)
    up(pl.ds((UP_CUTS - 1) * UP_CUT, 128))
    taps = taps_ref[...].astype(f32)

    def smooth(i, _):
        at = pl.multiple_of(i * 64, 64)
        v = up_ref[pl.ds(at, 64 + TOP), :].astype(f32)
        conv = v[TOP:] * taps[2:3, :]
        for back in (1, 2):
            conv = conv + pltpu.roll(v, back, 0)[TOP:] * taps[2 - back : 3 - back, :]
        act_ref[pl.ds(at, 64), :] = (gelu(conv[:, 0:UNITS]) * conv[:, UNITS:]).astype(bf16)
        return 0

    lax.fori_loop(0, ROWS // 64, smooth, 0)
    projected(act_ref, turned_ref, down_w, outs)


def ffn(operands):
    return pl.pallas_call(
        ffn_kernel,
        out_shape=PARTS,
        in_specs=[VMEM] * 8,
        out_specs=(VMEM,) * 4,
        scratch_shapes=[
            pltpu.VMEM((ROWS, D), bf16),
            pltpu.VMEM((ROWS + TOP, 2 * UNITS), bf16),
            pltpu.VMEM((ROWS, UNITS), bf16),
            pltpu.VMEM((ROWS, UNITS), bf16),
        ],
        compiler_params=pltpu.CompilerParams(vmem_limit_bytes=14 * 1024 * 1024),
        cost_estimate=pl.CostEstimate(
            flops=2 * ROWS * D * 3 * UNITS, bytes_accessed=13 * 1024 * 1024,
            transcendentals=ROWS * UNITS,
        ),
        name="ffn",
    )(*operands)


def shards(
    tokens, pre_mix_gain, w_gate_in, w_input, mix_kernel, w_recur, w_inject, decay_param,
    w_mix_out, post_mix_gain, pre_ffn_gain, w_up_gate, w_up_value, gate_kernel, value_kernel,
    w_down, post_ffn_gain,
):
    z_own = jnp.concatenate([w_gate_in, w_input, w_mix_out.T, w_down.T], axis=1)
    along_z = ring_gathered(z_own, "z", NZ)
    gains = jnp.concatenate([pre_mix_gain, post_mix_gain, pre_ffn_gain, post_ffn_gain])
    gains = gains.reshape(4, PIECE)
    packed = jnp.concatenate([tokens, jnp.pad(gains, ((0, EXTRA - 4), (0, 0)))], axis=0)
    mix_z, down_z = laid(along_z)
    mix_blocks = ring_gathered(mix_z, "x", NX)
    packed = jnp.stack([packed, swapped(packed)])
    x_blocks = rows_ring(packed)
    up_own = jnp.concatenate([w_up_gate, w_up_value], axis=1)
    sent = jnp.broadcast_to(up_own[None], (NX, *up_own.shape))
    along_x = lax.all_to_all(sent, "x", 0, 0, tiled=True)
    up_all = in_order(ring_gathered(along_x, "z", NZ), "z", 0).reshape(D, 2 * UNITS)
    down_all = in_order(ring_gathered(down_z, "x", NX), "x", 1).reshape(D, UNITS)
    x_blocks[1], decay_param = lax.optimization_barrier((x_blocks[1], decay_param))
    slope = jax.nn.softplus(-decay_param)[None, :]
    *parts, own_rows, gain_rows = mixer(
        (*x_blocks, *mix_blocks, mix_kernel, w_recur[0], w_inject[0], slope)
    )
    part = reduced_rows(*parts)
    part, taps_of = lax.optimization_barrier((part, (gate_kernel, value_kernel)))
    taps = jnp.concatenate(taps_of, axis=1)
    turned = swapped(jnp.concatenate([part[OWN:], part[:OWN]], axis=0))
    mixer_sum = part.astype(f32) + turned.astype(f32)
    middle = (own_rows.astype(f32) + row_normed(mixer_sum, gain_rows[1:2])).astype(bf16)
    normed = row_normed(middle.astype(f32), gain_rows[2:3]).astype(bf16).reshape(2, OWN, D)
    parts = ffn((*rows_ring(normed), up_all, down_all, taps))
    part = reduced_rows(*parts)
    ffn_sum = part[:OWN].astype(f32) + swapped(part[OWN:]).astype(f32)
    out_rows = middle[:OWN].astype(f32) + row_normed(ffn_sum, gain_rows[3:4])
    to_columns = out_rows.astype(bf16).reshape(OWN, NTP, PIECE).transpose(1, 0, 2)
    return lax.all_to_all(to_columns, TP, 0, 0, tiled=True).reshape(ROWS, PIECE)


def solution(mesh):
    finer = Mesh(mesh.devices.reshape(NZ, NX, NY, NC), ("z", "x", "y", "c"))
    return jax.shard_map(
        shards,
        mesh=finer,
        in_specs=(
            P(FS, TP), P(TP), P(FS, TP), P(FS, TP), P(None, TP), P(TP, None, None),
            P(TP, None, None), P(TP), P(TP, FS), P(TP), P(TP), P(FS, TP), P(FS, TP),
            P(None, TP), P(None, TP), P(TP, FS), P(TP),
        ),
        out_specs=P(FS, TP),
        check_vma=False,
    )
```
